32 devices in a mesh: sp: 8 (over z, y), tp: 4 (over x, core).
Axes of the slice: x: 2, y: 2, z: 4, core: 2. Of those that a mesh axis runs over, the one named last changes fastest.
Arguments:
- tokens: bfloat16 [2048, 2048], P(('sp', 'tp')), may hold values from -16 to 16
- w_query: bfloat16 [2048, 1024], P(None, 'tp'), may hold values from -1 to 1
- w_key: bfloat16 [2048, 256], P(None, 'tp'), may hold values from -1 to 1
- w_value: bfloat16 [2048, 256], P(None, 'tp'), may hold values from -0.125 to 0.125
- w_gate: bfloat16 [2048, 16], P(None, 'tp'), may hold values from -0.125 to 0.125
- gate_bias: float32 [16], P('tp'), as said below
- w_output: bfloat16 [1024, 2048], P('tp'), may hold values from -0.1875 to 0.1875
Outputs:
- mixed: bfloat16 [2048, 2048], P(('sp', 'tp'))
The draws below stay inside these ranges and needn't reach their ends.
Inputs may be any that keep to these rules, and one draw needn't show every extreme that they name: `gate_bias`: each head's forget gate bias is 4 or more; there is no upper bound.
All inputs are finite; a program needn't handle non-finite values.
Results may differ from the reference program's by a relative error of at most 0.012.
The reference program's roundings to bfloat16 on the way count: a program that leaves them out, or rounds other values in their place, can miss the bound.
Values may be sent and summed in bfloat16 or wider, within the bound.
A program may use at most 64 MiB of HBM per device.

```python
import math
import jax
import jax.numpy as jnp
from jax import lax

D = 2048
HEADS = 16
KV_HEADS = 4
HEAD = 64
TOK_DEV = 256
SEQ = 2048
N_TP = 4


def query_base(base_key):
    raw_values = jax.random.normal(jax.random.fold_in(base_key, 11), (D, HEADS * HEAD), jnp.float32)
    return jnp.clip(raw_values, -5.0, 5.0) / math.sqrt(D)


def draw_w_query(key, part):
    return query_base(key).astype(jnp.bfloat16)


def draw_w_key(key, part):
    raw_values = jax.random.normal(jax.random.fold_in(key, 12), (D, KV_HEADS * HEAD), jnp.float32)
    return (jnp.clip(raw_values, -5.0, 5.0) / math.sqrt(D)).astype(jnp.bfloat16)


def draw_gate_bias(key, part):
    shuffled = jax.random.permutation(jax.random.fold_in(key, 21), HEADS)
    quick = shuffled < HEADS // 2
    lasting = math.log(SEQ) + jax.random.uniform(jax.random.fold_in(key, 22), (HEADS,), jnp.float32, 0.5, 1.5)
    fading = jax.random.uniform(jax.random.fold_in(key, 23), (HEADS,), jnp.float32, 4.1, 5.3)
    return jnp.where(quick, fading, lasting).astype(jnp.float32)


def draw_tokens(key, part):
    span_rows = TOK_DEV // 2
    span_count = SEQ // span_rows
    scales = jnp.exp(jax.random.uniform(jax.random.fold_in(key, 31), (span_count, 1, 1), jnp.float32, math.log(0.6), math.log(1.6)))
    shifts = jax.random.uniform(jax.random.fold_in(key, 32), (span_count, 1, 1), jnp.float32, -1.5, 1.5)
    heading = jnp.clip(jax.random.normal(jax.random.fold_in(key, 33), (1, 1, D), jnp.float32), -3.0, 3.0)
    noise = jnp.clip(jax.random.normal(jax.random.fold_in(key, 34), (span_count, span_rows, D), jnp.float32), -5.0, 5.0)
    field = (scales * (noise + shifts * heading)).reshape(SEQ, D)
    return jnp.clip(field, -16.0, 16.0).astype(jnp.bfloat16)


def block_levels(stream_key, dims, pieces, low, largest):
    loudness = 1.0
    for axis_at, shards_of in pieces:
        steps = jax.random.uniform(jax.random.fold_in(jax.random.fold_in(stream_key, 6), axis_at), (shards_of,), jnp.float32, low / len(pieces), largest / len(pieces))
        loudness = loudness * jnp.repeat(jnp.exp(steps), dims[axis_at] // shards_of).reshape((-1,) + (1,) * (len(dims) - 1 - axis_at))
    return loudness


def normal_values(key, extent, deviation, reach, shards=(), kind=jnp.bfloat16):
    values = jax.random.normal(key, extent, jnp.float32) * deviation
    if len(shards) > 0:
        values = block_levels(key, extent, shards, -0.22, 0.18) * values
    return jnp.clip(values, min=-reach, max=reach).astype(kind)


def setup_inputs(seed: int = 0) -> dict:
    splits = jax.random.split(jax.random.key(seed), 8)
    return {
        "tokens": draw_tokens(jax.random.fold_in(splits[7], 71), 0),
        "w_query": draw_w_query(jax.random.fold_in(splits[7], 71), 0),
        "w_key": draw_w_key(jax.random.fold_in(splits[7], 71), 0),
        "w_value": normal_values(splits[3], (D, KV_HEADS * HEAD), D ** -0.5, 0.125, ((1, 4),)),
        "w_gate": normal_values(splits[4], (D, HEADS), D ** -0.5, 0.125, ((1, 4),)),
        "gate_bias": draw_gate_bias(jax.random.fold_in(splits[7], 71), 0),
        "w_output": normal_values(splits[6], (HEADS * HEAD, D), (HEADS * HEAD) ** -0.5, 0.1875, ((0, 4),)),
    }


masked_value = -1e30


def reference(tokens, w_query, w_key, w_value, w_gate, gate_bias, w_output):
    length = tokens.shape[0]
    group_size = HEADS // KV_HEADS
    queries = jnp.dot(tokens, w_query, preferred_element_type=jnp.float32).astype(jnp.bfloat16)
    key_proj = jnp.dot(tokens, w_key, preferred_element_type=jnp.float32).astype(jnp.bfloat16)
    value_proj = jnp.dot(tokens, w_value, preferred_element_type=jnp.float32).astype(jnp.bfloat16)
    gate_logits = jnp.dot(tokens, w_gate, preferred_element_type=jnp.float32).astype(jnp.bfloat16)
    queries, key_proj, value_proj, gate_logits = lax.optimization_barrier((queries, key_proj, value_proj, gate_logits))
    log_gates = jax.nn.log_sigmoid(gate_logits.astype(jnp.float32) + gate_bias.astype(jnp.float32))
    cumulative = jnp.cumsum(log_gates, axis=0)
    span = math.gcd(length, 512)
    block_total = length // span
    query_all = queries.astype(jnp.float32).reshape(block_total, span, KV_HEADS, group_size, HEAD)
    key_all = key_proj.astype(jnp.float32).reshape(block_total, span, KV_HEADS, HEAD)
    value_all = value_proj.astype(jnp.float32).reshape(block_total, span, KV_HEADS, HEAD)
    cumul_all = cumulative.reshape(block_total, span, KV_HEADS, group_size)
    scale = HEAD ** -0.5

    def query_block(block_index):
        query_here = lax.dynamic_index_in_dim(query_all, block_index, 0, keepdims=False)
        cumul_here = lax.dynamic_index_in_dim(cumul_all, block_index, 0, keepdims=False).transpose(1, 2, 0)
        query_position = block_index * span + jnp.arange(span, dtype=jnp.int32)

        def key_step(key_index, carry_state):
            row_peak, row_mass, row_accum = carry_state
            key_here = lax.dynamic_index_in_dim(key_all, key_index, 0, keepdims=False)
            value_here = lax.dynamic_index_in_dim(value_all, key_index, 0, keepdims=False)
            key_cumul = lax.dynamic_index_in_dim(cumul_all, key_index, 0, keepdims=False).transpose(1, 2, 0)
            key_position = key_index * span + jnp.arange(span, dtype=jnp.int32)
            scores = jnp.einsum("tkgd,skd->kgts", query_here, key_here) * scale
            scores = scores + cumul_here[:, :, :, None] - key_cumul[:, :, None, :]
            allowed = key_position[None, :] <= query_position[:, None]
            scores = jnp.where(allowed, scores, masked_value)
            new_peak = jnp.maximum(row_peak, jnp.max(scores, axis=3))
            weights = jnp.where(allowed, jnp.exp(scores - new_peak[:, :, :, None]), 0.0)
            rescale = jnp.exp(row_peak - new_peak)
            row_mass = row_mass * rescale + jnp.sum(weights, axis=3)
            weights_low = lax.optimization_barrier(weights.astype(jnp.bfloat16))
            row_accum = row_accum * rescale[:, :, :, None] + jnp.einsum(
                "kgts,skd->kgtd", weights_low.astype(jnp.float32), value_here)
            return new_peak, row_mass, row_accum

        initial = (jnp.full((KV_HEADS, group_size, span), masked_value, jnp.float32),
                   jnp.zeros((KV_HEADS, group_size, span), jnp.float32),
                   jnp.zeros((KV_HEADS, group_size, span, HEAD), jnp.float32))
        row_peak, row_mass, row_accum = lax.fori_loop(0, block_index + 1, key_step, initial)
        attended = (row_accum / row_mass[:, :, :, None]).astype(jnp.bfloat16)
        return attended.transpose(2, 0, 1, 3).reshape(span, HEADS * HEAD)

    attended = lax.map(query_block, jnp.arange(block_total, dtype=jnp.int32)).reshape(length, HEADS * HEAD)
    per_group = HEADS * HEAD // N_TP
    total = jnp.zeros((length, D), jnp.float32)
    for group_index in range(N_TP):
        partial_value = jnp.dot(attended[:, group_index * per_group:(group_index + 1) * per_group],
                          w_output[group_index * per_group:(group_index + 1) * per_group],
                          preferred_element_type=jnp.float32).astype(jnp.bfloat16)
        partial_value = lax.optimization_barrier(partial_value)
        total = total + partial_value.astype(jnp.float32)
    return total.astype(jnp.bfloat16)
```

```python
import functools

import jax
import jax.numpy as jnp
from jax import lax
from jax.experimental import pallas as pl
from jax.experimental.pallas import tpu as pltpu
from jax.sharding import PartitionSpec as P

HEAD = 64
LANES = 128
masked_value = -1e30
MESH = pl.DeviceIdType.MESH


def kernel(
    sp, tp, chunks, out_chunks,
    tokens, w_query, w_key, w_value, w_gate, bias, w_output,
    out,
    tok, w_all, w_k, w_v, w_g, wo, wo_pair, proj, qs, kv, cum,
    peak, mass, accum, att, att_pair, keep, outgoing, incoming,
    local_sem, own_sem, cross_send, cross_recv, pair_send, pair_recv, relay_send, relay_recv,
    wo_send, wo_recv, kv_send, kv_recv, cum_send, cum_recv,
    att_send, att_recv, out_send, out_recv,
):
    lo_n = 2
    hi_n = tp // lo_n
    me = lax.axis_index("sp")
    t_me = lax.axis_index("tp")
    hi, lo = lax.div(t_me, lo_n), lax.rem(t_me, lo_n)
    pair = hi * lo_n + (1 - lo)
    rows = tok.shape[1]
    local_rows = rows * tp
    width = tok.shape[2]
    q_cols = w_query.shape[1]
    heads = w_gate.shape[1]
    key_cols = w_key.shape[1]
    piece = width // chunks
    out_cols = w_output.shape[1]
    out_piece = out_cols // out_chunks

    def cross(d):
        return lax.rem(hi + d, hi_n) * lo_n + lo

    loads = [
        pltpu.make_async_copy(w_key, w_k, local_sem.at[0]),
        pltpu.make_async_copy(w_value, w_v, local_sem.at[1]),
        pltpu.make_async_copy(w_gate, w_g, local_sem.at[2]),
        pltpu.make_async_copy(w_query, w_all.at[:, pl.ds(0, q_cols)], local_sem.at[3]),
        pltpu.make_async_copy(w_output, wo, local_sem.at[4]),
    ]
    own = pltpu.make_async_copy(tokens, tok.at[t_me], own_sem)
    own.start()
    for load in loads:
        load.start()

    barrier = pltpu.get_barrier_semaphore()
    pl.semaphore_signal(barrier, inc=1, device_id={"tp": pair}, device_id_type=MESH)
    for d in range(1, hi_n):
        pl.semaphore_signal(barrier, inc=1, device_id={"tp": cross(d)}, device_id_type=MESH)

    def greet(d, carry):
        pl.semaphore_signal(
            barrier, inc=1, device_id={"sp": lax.rem(me + d, sp)}, device_id_type=MESH
        )
        return carry

    lax.fori_loop(1, sp, greet, 0)
    pl.semaphore_wait(barrier, 1 + (hi_n - 1) + (sp - 1))

    def cols(k):
        return pl.ds(k * piece, piece)

    def cross_copy(d, k):
        return pltpu.make_async_remote_copy(
            tokens.at[:, cols(k)], tok.at[t_me, :, cols(k)],
            cross_send.at[d - 1, k], cross_recv.at[d - 1, k],
            device_id={"tp": cross(d)}, device_id_type=MESH,
        )

    def pair_copy(k):
        return pltpu.make_async_remote_copy(
            tokens.at[:, cols(k)], tok.at[t_me, :, cols(k)],
            pair_send.at[k], pair_recv.at[k],
            device_id={"tp": pair}, device_id_type=MESH,
        )

    def relay_copy(d, k):
        source = lax.rem(hi - d + hi_n, hi_n) * lo_n + lo
        return pltpu.make_async_remote_copy(
            tok.at[source, :, cols(k)], tok.at[source, :, cols(k)],
            relay_send.at[d - 1, k], relay_recv.at[d - 1, k],
            device_id={"tp": pair}, device_id_type=MESH,
        )

    for k in range(chunks):
        for d in range(1, hi_n):
            cross_copy(d, k).start()
    for k in range(chunks):
        pair_copy(k).start()

    for load in loads[:3]:
        load.wait()
    build = 256

    def assemble(i, carry):
        span = pl.ds(pl.multiple_of(i * build, build), build)
        w_all[span, q_cols:q_cols + LANES] = jnp.concatenate([w_k[span, :], w_v[span, :]], axis=1)
        w_all[span, q_cols + LANES:] = jnp.concatenate(
            [w_g[span, :], jnp.zeros((build, LANES - heads), jnp.bfloat16)], axis=1
        )
        return carry

    lax.fori_loop(0, width // build, assemble, 0)
    loads[3].wait()
    loads[4].wait()
    own.wait()
    wo_copy = pltpu.make_async_remote_copy(
        wo, wo_pair, wo_send, wo_recv, device_id={"tp": pair}, device_id_type=MESH
    )

    for k in range(chunks):
        for d in range(1, hi_n):
            cross_copy(d, k).wait_recv()
            relay_copy(d, k).start()
        pair_copy(k).wait_recv()
        for d in range(1, hi_n):
            relay_copy(d, k).wait_recv()
        here = tok[:, :, k * piece:(k + 1) * piece].reshape(local_rows, piece)
        part = jnp.dot(here, w_all[k * piece:(k + 1) * piece, :], preferred_element_type=jnp.float32)
        if k == 0:
            proj[...] = part
        else:
            proj[...] += part
    wo_copy.start()

    kv[me] = proj[:, q_cols:q_cols + 2 * key_cols].astype(jnp.bfloat16)
    scale = HEAD ** -0.5
    for h in range(heads):
        q = proj[:, h * HEAD:(h + 1) * HEAD].astype(jnp.bfloat16) * jnp.bfloat16(scale)
        qs[h] = jnp.concatenate([q, jnp.zeros((local_rows, LANES - HEAD), jnp.bfloat16)], axis=1)

    def kv_copy(d):
        return pltpu.make_async_remote_copy(
            kv.at[me], kv.at[me], kv_send.at[d], kv_recv.at[me],
            device_id={"sp": d}, device_id_type=MESH,
        )

    def cum_copy(d):
        return pltpu.make_async_remote_copy(
            cum.at[me], cum.at[me], cum_send.at[d], cum_recv.at[me],
            device_id={"sp": d}, device_id_type=MESH,
        )

    def arrival(r):
        return (
            pltpu.make_async_remote_copy(
                kv.at[r], kv.at[r], kv_send.at[r], kv_recv.at[r],
                device_id={"sp": r}, device_id_type=MESH,
            ),
            pltpu.make_async_remote_copy(
                cum.at[r], cum.at[r], cum_send.at[r], cum_recv.at[r],
                device_id={"sp": r}, device_id_type=MESH,
            ),
        )

    later = sp - 1 - me

    def send_kv(i, carry):
        kv_copy(sp - 1 - i).start()
        return carry

    def send_cum(i, carry):
        cum_copy(sp - 1 - i).start()
        return carry

    lax.fori_loop(0, later, send_kv, 0)

    logits = proj[:, q_cols + LANES:].astype(jnp.bfloat16).astype(jnp.float32).T[:8, :]
    u = logits + bias[...]
    gates = jnp.minimum(u, 0.0) - jnp.log1p(jnp.exp(-jnp.abs(u)))
    upper = (
        lax.broadcasted_iota(jnp.int32, (local_rows, local_rows), 0)
        <= lax.broadcasted_iota(jnp.int32, (local_rows, local_rows), 1)
    )
    ones = jnp.where(upper, 1.0, 0.0).astype(jnp.bfloat16)
    g0 = gates.astype(jnp.bfloat16)
    r1 = gates - g0.astype(jnp.float32)
    g1 = r1.astype(jnp.bfloat16)
    g2 = (r1 - g1.astype(jnp.float32)).astype(jnp.bfloat16)
    total = jnp.dot(g2, ones, preferred_element_type=jnp.float32)
    total = total + jnp.dot(g1, ones, preferred_element_type=jnp.float32)
    total = total + jnp.dot(g0, ones, preferred_element_type=jnp.float32)
    cum[me] = total
    lax.fori_loop(0, later, send_cum, 0)

    halves = local_rows // LANES

    def lane_parts(x):
        return [x[:, j * LANES:(j + 1) * LANES] for j in range(halves)]

    def attend(h, kv_here, bias_row, first):
        s = lax.dot_general(
            qs[h], kv_here, (((1,), (1,)), ((), ())), preferred_element_type=jnp.float32
        ) + bias_row
        if first:
            allowed = (
                lax.broadcasted_iota(jnp.int32, (local_rows, local_rows), 1)
                <= lax.broadcasted_iota(jnp.int32, (local_rows, local_rows), 0)
            )
            s = jnp.where(allowed, s, masked_value)
        top = jnp.max(s, axis=1, keepdims=True)
        if first:
            new_peak = jnp.broadcast_to(top, (local_rows, LANES))
        else:
            old_peak = peak[h]
            new_peak = jnp.maximum(old_peak, top)
        p = [jnp.exp(x - new_peak) for x in lane_parts(s)]
        p_sum = functools.reduce(lambda a, b: a + b, p)
        weights = jnp.concatenate([x.astype(jnp.bfloat16) for x in p], axis=1)
        term = jnp.dot(weights, kv_here, preferred_element_type=jnp.float32)
        peak[h] = new_peak
        if first:
            mass[h] = p_sum
            accum[h] = term
        else:
            rescale = jnp.exp(old_peak - new_peak)
            mass[h] = mass[h] * rescale + p_sum
            accum[h] = accum[h] * rescale + term

    for h in range(heads):
        attend(h, kv[me], -total[h:h + 1, :], True)

    def one_block(i, base):
        r = me - 1 - i
        for copy in arrival(r):
            copy.wait_recv()
        cum_here = cum[r]
        base = base + cum_here[:, local_rows - 1:]
        shift = base - cum_here
        kv_here = kv[r]
        for h in range(heads):
            attend(h, kv_here, shift[h:h + 1, :], False)
        return base

    lax.fori_loop(0, me, one_block, jnp.zeros((8, 1), jnp.float32))

    for h in range(heads):
        denominator = jnp.sum(mass[h], axis=1, keepdims=True)
        done = (accum[h][:, key_cols:2 * key_cols] / denominator).astype(jnp.bfloat16)
        att[:, :, :, h * HEAD:(h + 1) * HEAD] = done.reshape(hi_n, lo_n, rows, HEAD)

    def att_copy(d):
        return pltpu.make_async_remote_copy(
            att.at[d, 1 - lo], att_pair.at[d], att_send.at[d], att_recv.at[d],
            device_id={"tp": pair}, device_id_type=MESH,
        )

    for d in range(hi_n):
        att_copy(d).start()
    wo_copy.wait_recv()
    for d in range(hi_n):
        att_copy(d).wait_recv()
    mine = att[:, lo].reshape(hi_n * rows, q_cols)
    theirs = att_pair[...].reshape(hi_n * rows, q_cols)

    def out_copy(d, k):
        span = pl.ds(k * out_piece, out_piece)
        return pltpu.make_async_remote_copy(
            outgoing.at[lax.rem(hi + d, hi_n), :, span], incoming.at[d - 1, :, span],
            out_send.at[d - 1, k], out_recv.at[d - 1, k],
            device_id={"tp": cross(d)}, device_id_type=MESH,
        )

    for k in range(out_chunks):
        span = slice(k * out_piece, (k + 1) * out_piece)
        a = jnp.dot(mine, wo[:, span], preferred_element_type=jnp.float32).astype(jnp.bfloat16)
        b = jnp.dot(theirs, wo_pair[:, span], preferred_element_type=jnp.float32).astype(jnp.bfloat16)
        both = a.astype(jnp.float32) + b.astype(jnp.float32)
        keep[:, :, span] = both.reshape(hi_n, rows, out_piece)
        outgoing[:, :, span] = both.astype(jnp.bfloat16).reshape(hi_n, rows, out_piece)
        for d in range(1, hi_n):
            out_copy(d, k).start()
    for k in range(out_chunks):
        span = slice(k * out_piece, (k + 1) * out_piece)
        value = keep[hi, :, span]
        for d in range(1, hi_n):
            out_copy(d, k).wait_recv()
            value = value + incoming[d - 1, :, span].astype(jnp.float32)
        out[:, span] = value.astype(jnp.bfloat16)

    for k in range(chunks):
        for d in range(1, hi_n):
            cross_copy(d, k).wait_send()
            relay_copy(d, k).wait_send()
        pair_copy(k).wait_send()
    wo_copy.wait_send()
    for d in range(hi_n):
        att_copy(d).wait_send()
    for k in range(out_chunks):
        for d in range(1, hi_n):
            out_copy(d, k).wait_send()

    def drain(i, carry):
        kv_copy(sp - 1 - i).wait_send()
        cum_copy(sp - 1 - i).wait_send()
        return carry

    lax.fori_loop(0, later, drain, 0)


def shards(tokens, w_query, w_key, w_value, w_gate, gate_bias, w_output):
    sp = lax.axis_size("sp")
    tp = lax.axis_size("tp")
    rows, width = tokens.shape
    local_rows = rows * tp
    q_cols, key_cols, heads = w_query.shape[1], w_key.shape[1], w_gate.shape[1]
    out_cols = w_output.shape[1]
    assert tp % 2 == 0 and 2 * key_cols == LANES and key_cols == HEAD and heads <= 8
    hi_n = tp // 2
    chunks = 4
    out_chunks = 4
    bias = jnp.pad(gate_bias, (0, 8 - heads), constant_values=4.0)[:, None]
    bf, f32 = jnp.bfloat16, jnp.float32
    dma = pltpu.SemaphoreType.DMA
    any_spec = pl.BlockSpec(memory_space=pl.ANY)
    vmem_spec = pl.BlockSpec(memory_space=pltpu.VMEM)
    return pl.pallas_call(
        functools.partial(kernel, sp, tp, chunks, out_chunks),
        out_shape=jax.ShapeDtypeStruct((rows, out_cols), bf),
        in_specs=[any_spec] * 5 + [vmem_spec, any_spec],
        out_specs=vmem_spec,
        scratch_shapes=[
            pltpu.VMEM((tp, rows, width), bf),
            pltpu.VMEM((width, q_cols + 2 * LANES), bf),
            pltpu.VMEM(w_key.shape, bf),
            pltpu.VMEM(w_value.shape, bf),
            pltpu.VMEM(w_gate.shape, bf),
            pltpu.VMEM(w_output.shape, bf),
            pltpu.VMEM(w_output.shape, bf),
            pltpu.VMEM((local_rows, q_cols + 2 * LANES), f32),
            pltpu.VMEM((heads, local_rows, LANES), bf),
            pltpu.VMEM((sp, local_rows, LANES), bf),
            pltpu.VMEM((sp, 8, local_rows), f32),
            pltpu.VMEM((heads, local_rows, LANES), f32),
            pltpu.VMEM((heads, local_rows, LANES), f32),
            pltpu.VMEM((heads, local_rows, LANES), f32),
            pltpu.VMEM((hi_n, 2, rows, q_cols), bf),
            pltpu.VMEM((hi_n, rows, q_cols), bf),
            pltpu.VMEM((hi_n, rows, out_cols), f32),
            pltpu.VMEM((hi_n, rows, out_cols), bf),
            pltpu.VMEM((max(hi_n - 1, 1), rows, out_cols), bf),
            dma((5,)),
            dma,
            dma((hi_n - 1, chunks)),
            dma((hi_n - 1, chunks)),
            dma((chunks,)),
            dma((chunks,)),
            dma((hi_n - 1, chunks)),
            dma((hi_n - 1, chunks)),
            dma,
            dma,
            dma((sp,)),
            dma((sp,)),
            dma((sp,)),
            dma((sp,)),
            dma((hi_n,)),
            dma((hi_n,)),
            dma((hi_n - 1, out_chunks)),
            dma((hi_n - 1, out_chunks)),
        ],
        compiler_params=pltpu.CompilerParams(
            collective_id=0, has_side_effects=True, vmem_limit_bytes=56 * 1024 * 1024
        ),
    )(tokens, w_query, w_key, w_value, w_gate, bias, w_output)


def solution(mesh):
    return jax.shard_map(
        shards,
        mesh=mesh,
        in_specs=(
            P(("sp", "tp"), None),
            P(None, "tp"),
            P(None, "tp"),
            P(None, "tp"),
            P(None, "tp"),
            P("tp"),
            P("tp", None),
        ),
        out_specs=P(("sp", "tp"), None),
        check_vma=False,
    )
```

```python
import functools

import jax
import jax.numpy as jnp
from jax import lax
from jax.experimental import pallas as pl
from jax.experimental.pallas import tpu as pltpu
from jax.sharding import PartitionSpec as P

HEAD = 64
LANES = 128
masked_value = -1e30
MESH = pl.DeviceIdType.MESH


def kernel(
    sp, tp, chunks, out_chunks,
    tokens, w_query, w_key, w_value, w_gate, bias, w_output,
    out,
    tok, w_all, w_kv, w_g, wo, wo_pair, proj, logits, qs, kv, cum, own_sum, pair_sum,
    peak, mass, accum, att, att_pair, keep, outgoing, incoming,
    local_sem, own_sem, cross_send, cross_recv, pair_send, pair_recv, relay_send, relay_recv,
    wo_send, wo_recv, kv_send, kv_recv, cum_send, cum_recv,
    kv_side, cum_side, sum_send, sum_recv,
    att_send, att_recv, out_send, out_recv,
):
    lo_n = 2
    hi_n = tp // lo_n
    me = lax.axis_index("sp")
    t_me = lax.axis_index("tp")
    hi, lo = lax.div(t_me, lo_n), lax.rem(t_me, lo_n)
    pair = hi * lo_n + (1 - lo)
    rows = tok.shape[1]
    local_rows = rows * tp
    width = tok.shape[2]
    q_cols = w_query.shape[1]
    heads = w_gate.shape[0]
    key_cols = w_key.shape[0]
    span_n = 2
    far_n = sp // span_n
    far, side = lax.div(me, span_n), lax.rem(me, span_n)
    mate = far * span_n + (1 - side)
    piece = width // chunks
    out_cols = w_output.shape[1]
    out_piece = out_cols // out_chunks

    def cross(d):
        return lax.rem(hi + d, hi_n) * lo_n + lo

    loads = [
        pltpu.make_async_copy(w_key, w_kv.at[pl.ds(0, key_cols)], local_sem.at[0]),
        pltpu.make_async_copy(w_value, w_kv.at[pl.ds(key_cols, key_cols)], local_sem.at[1]),
        pltpu.make_async_copy(w_gate, w_g, local_sem.at[2]),
        pltpu.make_async_copy(w_query, w_all.at[:, pl.ds(0, q_cols)], local_sem.at[3]),
        pltpu.make_async_copy(w_output, wo, local_sem.at[4]),
    ]
    own = pltpu.make_async_copy(tokens, tok.at[t_me], own_sem)
    own.start()
    for load in loads:
        load.start()

    barrier = pltpu.get_barrier_semaphore()
    pl.semaphore_signal(barrier, inc=1, device_id={"tp": pair}, device_id_type=MESH)
    for d in range(1, hi_n):
        pl.semaphore_signal(barrier, inc=1, device_id={"tp": cross(d)}, device_id_type=MESH)

    def greet(d, carry):
        other = lax.rem(far + d, far_n) * span_n + side
        pl.semaphore_signal(barrier, inc=1, device_id={"sp": other}, device_id_type=MESH)
        return carry

    lax.fori_loop(1, far_n, greet, 0)
    pl.semaphore_signal(barrier, inc=1, device_id={"sp": mate}, device_id_type=MESH)
    pl.semaphore_wait(barrier, 1 + (hi_n - 1) + (far_n - 1) + 1)

    def cols(k):
        return pl.ds(k * piece, piece)

    def cross_copy(d, k):
        return pltpu.make_async_remote_copy(
            tokens.at[:, cols(k)], tok.at[t_me, :, cols(k)],
            cross_send.at[d - 1, k], cross_recv.at[d - 1, k],
            device_id={"tp": cross(d)}, device_id_type=MESH,
        )

    def pair_copy(k):
        return pltpu.make_async_remote_copy(
            tokens.at[:, cols(k)], tok.at[t_me, :, cols(k)],
            pair_send.at[k], pair_recv.at[k],
            device_id={"tp": pair}, device_id_type=MESH,
        )

    def relay_copy(d, k):
        source = lax.rem(hi - d + hi_n, hi_n) * lo_n + lo
        return pltpu.make_async_remote_copy(
            tok.at[source, :, cols(k)], tok.at[source, :, cols(k)],
            relay_send.at[d - 1, k], relay_recv.at[d - 1, k],
            device_id={"tp": pair}, device_id_type=MESH,
        )

    for k in range(chunks):
        for d in range(1, hi_n):
            cross_copy(d, k).start()
    for k in range(chunks):
        pair_copy(k).start()

    for load in loads[:3]:
        load.wait()
    build = 256

    def assemble(i, carry):
        span = pl.ds(pl.multiple_of(i * build, build), build)
        w_all[span, q_cols:] = w_kv[:, span].T
        return carry

    lax.fori_loop(0, width // build, assemble, 0)
    loads[3].wait()
    loads[4].wait()
    own.wait()
    wo_copy = pltpu.make_async_remote_copy(
        wo, wo_pair, wo_send, wo_recv, device_id={"tp": pair}, device_id_type=MESH
    )

    for k in range(chunks):
        for d in range(1, hi_n):
            cross_copy(d, k).wait_recv()
            relay_copy(d, k).start()
        pair_copy(k).wait_recv()
        for d in range(1, hi_n):
            relay_copy(d, k).wait_recv()
        here = tok[:, :, k * piece:(k + 1) * piece].reshape(local_rows, piece)
        part = jnp.dot(here, w_all[k * piece:(k + 1) * piece, :], preferred_element_type=jnp.float32)
        gate_part = lax.dot_general(
            w_g[:, k * piece:(k + 1) * piece], here, (((1,), (1,)), ((), ())),
            preferred_element_type=jnp.float32,
        )
        if k == 0:
            proj[...] = part
            logits[0:heads, :] = gate_part
        else:
            proj[...] += part
            logits[0:heads, :] += gate_part
    wo_copy.start()

    kv[me] = proj[:, q_cols:q_cols + 2 * key_cols].astype(jnp.bfloat16)
    scale = HEAD ** -0.5
    for h in range(heads):
        q = proj[:, h * HEAD:(h + 1) * HEAD].astype(jnp.bfloat16) * jnp.bfloat16(scale)
        qs[h] = jnp.concatenate([q, jnp.zeros((local_rows, LANES - HEAD), jnp.bfloat16)], axis=1)

    def column(d):
        return (
            pltpu.make_async_remote_copy(
                kv.at[me], kv.at[me], kv_send.at[d], kv_recv.at[me],
                device_id={"sp": d * span_n + side}, device_id_type=MESH,
            ),
            pltpu.make_async_remote_copy(
                cum.at[me], cum.at[me], cum_send.at[d], cum_recv.at[me],
                device_id={"sp": d * span_n + side}, device_id_type=MESH,
            ),
        )

    def across(r):
        return (
            pltpu.make_async_remote_copy(
                kv.at[r], kv.at[r], kv_side.at[lax.div(r, span_n)], kv_recv.at[r],
                device_id={"sp": mate}, device_id_type=MESH,
            ),
            pltpu.make_async_remote_copy(
                cum.at[r], cum.at[r], cum_side.at[lax.div(r, span_n)], cum_recv.at[r],
                device_id={"sp": mate}, device_id_type=MESH,
            ),
        )

    later = far_n - 1 - far

    def send_column(which, i, carry):
        column(far_n - 1 - i)[which].start()
        return carry

    lax.fori_loop(0, later, functools.partial(send_column, 0), 0)

    @pl.when(side == 0)
    def _():
        across(me)[0].start()

    row_of = lax.broadcasted_iota(jnp.int32, (8, local_rows), 0)
    u = jnp.where(row_of < heads, logits[...].astype(jnp.bfloat16).astype(jnp.float32), 0.0)
    for h in range(heads):
        u = jnp.where(row_of == h, u + bias[h], u)
    gates = jnp.minimum(u, 0.0) - jnp.log1p(jnp.exp(-jnp.abs(u)))
    upper = (
        lax.broadcasted_iota(jnp.int32, (local_rows, local_rows), 0)
        <= lax.broadcasted_iota(jnp.int32, (local_rows, local_rows), 1)
    )
    ones = jnp.where(upper, 1.0, 0.0).astype(jnp.bfloat16)
    g0 = gates.astype(jnp.bfloat16)
    r1 = gates - g0.astype(jnp.float32)
    g1 = r1.astype(jnp.bfloat16)
    g2 = (r1 - g1.astype(jnp.float32)).astype(jnp.bfloat16)
    total = jnp.dot(g2, ones, preferred_element_type=jnp.float32)
    total = total + jnp.dot(g1, ones, preferred_element_type=jnp.float32)
    total = total + jnp.dot(g0, ones, preferred_element_type=jnp.float32)
    own_sum[...] = jnp.broadcast_to(total[:, local_rows - 1:], (8, LANES))
    sum_copy = pltpu.make_async_remote_copy(
        own_sum, pair_sum, sum_send, sum_recv, device_id={"sp": mate}, device_id_type=MESH
    )
    sum_copy.start()
    sum_copy.wait_recv()
    other_sum = pair_sum[...]
    start = jnp.where(side == 1, other_sum[:, :1], 0.0)
    total = total + start
    cum[me, :, 0:local_rows] = total
    cum[me, :, local_rows:] = own_sum[...] + other_sum
    lax.fori_loop(0, later, functools.partial(send_column, 1), 0)

    @pl.when(side == 0)
    def _():
        across(me)[1].start()

    halves = local_rows // LANES

    def lane_parts(x):
        return [x[:, j * LANES:(j + 1) * LANES] for j in range(halves)]

    def attend(h, kv_here, bias_row, first):
        s = lax.dot_general(
            qs[h], kv_here, (((1,), (1,)), ((), ())), preferred_element_type=jnp.float32
        ) + bias_row
        if first:
            allowed = (
                lax.broadcasted_iota(jnp.int32, (local_rows, local_rows), 1)
                <= lax.broadcasted_iota(jnp.int32, (local_rows, local_rows), 0)
            )
            s = jnp.where(allowed, s, masked_value)
        top = jnp.max(s, axis=1, keepdims=True)
        if first:
            new_peak = jnp.broadcast_to(top, (local_rows, LANES))
        else:
            old_peak = peak[h]
            new_peak = jnp.maximum(old_peak, top)
        p = [jnp.exp(x - new_peak) for x in lane_parts(s)]
        p_sum = functools.reduce(lambda a, b: a + b, p)
        weights = jnp.concatenate([x.astype(jnp.bfloat16) for x in p], axis=1)
        term = jnp.dot(weights, kv_here, preferred_element_type=jnp.float32)
        peak[h] = new_peak
        if first:
            mass[h] = p_sum
            accum[h] = term
        else:
            rescale = jnp.exp(old_peak - new_peak)
            mass[h] = mass[h] * rescale + p_sum
            accum[h] = accum[h] * rescale + term

    for h in range(heads):
        attend(h, kv[me], -total[h:h + 1, :], True)

    def block_of(r, base):
        kv_here = kv[r]
        shift = base - cum[r, :, 0:local_rows]
        for h in range(heads):
            attend(h, kv_here, shift[h:h + 1, :], False)

    def same_side(i, base):
        r = (far - 1 - i) * span_n + side
        for copy in across(r):
            copy.wait_recv()
        for copy in across(r):
            copy.start()
        base = base + cum[r, :, local_rows:local_rows + 1]
        block_of(r, base)
        return base

    zero = jnp.zeros((8, 1), jnp.float32)
    lax.fori_loop(0, far, same_side, zero)

    @pl.when(side == 1)
    def _():
        for copy in across(mate):
            copy.wait_recv()
        block_of(mate, zero)

    def other_side(i, base):
        r = (far - 1 - i) * span_n + 1 - side
        for copy in across(r):
            copy.wait_recv()
        base = base + cum[r, :, local_rows:local_rows + 1]
        block_of(r, base)
        return base

    lax.fori_loop(0, far, other_side, zero)

    for h in range(heads):
        denominator = jnp.sum(mass[h], axis=1, keepdims=True)
        done = (accum[h][:, key_cols:2 * key_cols] / denominator).astype(jnp.bfloat16)
        att[:, :, :, h * HEAD:(h + 1) * HEAD] = done.reshape(hi_n, lo_n, rows, HEAD)

    def att_copy(d):
        return pltpu.make_async_remote_copy(
            att.at[d, 1 - lo], att_pair.at[d], att_send.at[d], att_recv.at[d],
            device_id={"tp": pair}, device_id_type=MESH,
        )

    for d in range(hi_n):
        att_copy(d).start()
    wo_copy.wait_recv()
    for d in range(hi_n):
        att_copy(d).wait_recv()
    mine = att[:, lo].reshape(hi_n * rows, q_cols)
    theirs = att_pair[...].reshape(hi_n * rows, q_cols)

    def out_copy(d, k):
        span = pl.ds(k * out_piece, out_piece)
        return pltpu.make_async_remote_copy(
            outgoing.at[lax.rem(hi + d, hi_n), :, span], incoming.at[d - 1, :, span],
            out_send.at[d - 1, k], out_recv.at[d - 1, k],
            device_id={"tp": cross(d)}, device_id_type=MESH,
        )

    for k in range(out_chunks):
        span = slice(k * out_piece, (k + 1) * out_piece)
        a = jnp.dot(mine, wo[:, span], preferred_element_type=jnp.float32).astype(jnp.bfloat16)
        b = jnp.dot(theirs, wo_pair[:, span], preferred_element_type=jnp.float32).astype(jnp.bfloat16)
        both = a.astype(jnp.float32) + b.astype(jnp.float32)
        keep[:, :, span] = both.reshape(hi_n, rows, out_piece)
        outgoing[:, :, span] = both.astype(jnp.bfloat16).reshape(hi_n, rows, out_piece)
        for d in range(1, hi_n):
            out_copy(d, k).start()
    for k in range(out_chunks):
        span = slice(k * out_piece, (k + 1) * out_piece)
        value = keep[hi, :, span]
        for d in range(1, hi_n):
            out_copy(d, k).wait_recv()
            value = value + incoming[d - 1, :, span].astype(jnp.float32)
        out[:, span] = value.astype(jnp.bfloat16)

    for k in range(chunks):
        for d in range(1, hi_n):
            cross_copy(d, k).wait_send()
            relay_copy(d, k).wait_send()
        pair_copy(k).wait_send()
    wo_copy.wait_send()
    for d in range(hi_n):
        att_copy(d).wait_send()
    for k in range(out_chunks):
        for d in range(1, hi_n):
            out_copy(d, k).wait_send()

    sum_copy.wait_send()

    @pl.when(side == 0)
    def _():
        for copy in across(me):
            copy.wait_send()

    def drain(i, carry):
        for copy in column(far_n - 1 - i):
            copy.wait_send()
        return carry

    lax.fori_loop(0, later, drain, 0)

    def drain_side(i, carry):
        for copy in across((far - 1 - i) * span_n + side):
            copy.wait_send()
        return carry

    lax.fori_loop(0, far, drain_side, 0)


def shards(tokens, w_query, w_key, w_value, w_gate, gate_bias, w_output):
    sp = lax.axis_size("sp")
    tp = lax.axis_size("tp")
    rows, width = tokens.shape
    local_rows = rows * tp
    q_cols, key_cols, heads = w_query.shape[1], w_key.shape[1], w_gate.shape[1]
    out_cols = w_output.shape[1]
    assert tp % 2 == 0 and sp % 2 == 0 and 2 * key_cols == LANES and key_cols == HEAD and heads <= 8
    hi_n = tp // 2
    chunks = 4
    out_chunks = 4
    bf, f32 = jnp.bfloat16, jnp.float32
    dma = pltpu.SemaphoreType.DMA
    any_spec = pl.BlockSpec(memory_space=pl.ANY)
    vmem_spec = pl.BlockSpec(memory_space=pltpu.VMEM)
    return pl.pallas_call(
        functools.partial(kernel, sp, tp, chunks, out_chunks),
        out_shape=jax.ShapeDtypeStruct((rows, out_cols), bf),
        in_specs=[any_spec] * 5 + [pl.BlockSpec(memory_space=pltpu.SMEM), any_spec],
        out_specs=vmem_spec,
        scratch_shapes=[
            pltpu.VMEM((tp, rows, width), bf),
            pltpu.VMEM((width, q_cols + LANES), bf),
            pltpu.VMEM((LANES, width), bf),
            pltpu.VMEM((heads, width), bf),
            pltpu.VMEM(w_output.shape, bf),
            pltpu.VMEM(w_output.shape, bf),
            pltpu.VMEM((local_rows, q_cols + LANES), f32),
            pltpu.VMEM((8, local_rows), f32),
            pltpu.VMEM((heads, local_rows, LANES), bf),
            pltpu.VMEM((sp, local_rows, LANES), bf),
            pltpu.VMEM((sp, 8, local_rows + LANES), f32),
            pltpu.VMEM((8, LANES), f32),
            pltpu.VMEM((8, LANES), f32),
            pltpu.VMEM((heads, local_rows, LANES), f32),
            pltpu.VMEM((heads, local_rows, LANES), f32),
            pltpu.VMEM((heads, local_rows, LANES), f32),
            pltpu.VMEM((hi_n, 2, rows, q_cols), bf),
            pltpu.VMEM((hi_n, rows, q_cols), bf),
            pltpu.VMEM((hi_n, rows, out_cols), f32),
            pltpu.VMEM((hi_n, rows, out_cols), bf),
            pltpu.VMEM((max(hi_n - 1, 1), rows, out_cols), bf),
            dma((5,)),
            dma,
            dma((hi_n - 1, chunks)),
            dma((hi_n - 1, chunks)),
            dma((chunks,)),
            dma((chunks,)),
            dma((hi_n - 1, chunks)),
            dma((hi_n - 1, chunks)),
            dma,
            dma,
            dma((sp // 2,)),
            dma((sp,)),
            dma((sp // 2,)),
            dma((sp,)),
            dma((sp // 2,)),
            dma((sp // 2,)),
            dma,
            dma,
            dma((hi_n,)),
            dma((hi_n,)),
            dma((hi_n - 1, out_chunks)),
            dma((hi_n - 1, out_chunks)),
        ],
        compiler_params=pltpu.CompilerParams(
            collective_id=0, has_side_effects=True, vmem_limit_bytes=(20 << 20) + (sp << 17)
        ),
    )(tokens, w_query, w_key.T, w_value.T, w_gate.T, gate_bias, w_output)


def solution(mesh):
    return jax.shard_map(
        shards,
        mesh=mesh,
        in_specs=(
            P(("sp", "tp"), None),
            P(None, "tp"),
            P(None, "tp"),
            P(None, "tp"),
            P(None, "tp"),
            P("tp"),
            P("tp", None),
        ),
        out_specs=P(("sp", "tp"), None),
        check_vma=False,
    )
```

```python
import functools

import jax
import jax.numpy as jnp
from jax import lax
from jax.experimental import pallas as pl
from jax.experimental.pallas import tpu as pltpu
from jax.sharding import PartitionSpec as P

HEAD = 64
LANES = 128
masked_value = -1e30
MESH = pl.DeviceIdType.MESH


def kernel(
    sp, tp, chunks, out_chunks,
    tokens, w_query, w_key, w_value, w_gate, bias_in, w_output,
    out,
    tok, w_all, w_kv, w_g, wo, wo_pair, proj, logits, qs, kv, cum, own_sum, pair_sum,
    peak, mass, accum, att, att_pair, keep, outgoing, incoming, bias,
    local_sem, own_sem, cross_send, cross_recv, pair_send, pair_recv, relay_send, relay_recv,
    wo_send, wo_recv, kv_send, kv_recv, cum_send, cum_recv,
    kv_side, cum_side, sum_send, sum_recv,
    att_send, att_recv, out_send, out_recv,
):
    lo_n = 2
    hi_n = tp // lo_n
    me = lax.axis_index("sp")
    t_me = lax.axis_index("tp")
    hi, lo = lax.div(t_me, lo_n), lax.rem(t_me, lo_n)
    pair = hi * lo_n + (1 - lo)
    rows = tok.shape[1]
    local_rows = rows * tp
    width = tok.shape[2]
    q_cols = w_query.shape[1]
    heads = w_gate.shape[0]
    key_cols = w_key.shape[0]
    span_n = 2
    far_n = sp // span_n
    far, side = lax.div(me, span_n), lax.rem(me, span_n)
    mate = far * span_n + (1 - side)
    piece = width // chunks
    out_cols = w_output.shape[1]
    out_piece = out_cols // out_chunks
    group = lo_n * rows

    def cross(d):
        return lax.rem(hi + d, hi_n) * lo_n + lo

    loads = [
        pltpu.make_async_copy(w_key, w_kv.at[pl.ds(0, key_cols)], local_sem.at[0]),
        pltpu.make_async_copy(w_value, w_kv.at[pl.ds(key_cols, key_cols)], local_sem.at[1]),
        pltpu.make_async_copy(w_gate, w_g, local_sem.at[2]),
        pltpu.make_async_copy(w_query, w_all.at[:, pl.ds(0, q_cols)], local_sem.at[3]),
        pltpu.make_async_copy(w_output, wo, local_sem.at[4]),
        pltpu.make_async_copy(bias_in, bias, local_sem.at[5]),
    ]
    own = pltpu.make_async_copy(tokens, tok.at[t_me], own_sem)
    own.start()
    for load in loads:
        load.start()

    barrier = pltpu.get_barrier_semaphore()
    pl.semaphore_signal(barrier, inc=1, device_id={"tp": pair}, device_id_type=MESH)
    for d in range(1, hi_n):
        pl.semaphore_signal(barrier, inc=1, device_id={"tp": cross(d)}, device_id_type=MESH)

    def greet(d, carry):
        other = lax.rem(far + d, far_n) * span_n + side
        pl.semaphore_signal(barrier, inc=1, device_id={"sp": other}, device_id_type=MESH)
        return carry

    lax.fori_loop(1, far_n, greet, 0)
    pl.semaphore_signal(barrier, inc=1, device_id={"sp": mate}, device_id_type=MESH)
    pl.semaphore_wait(barrier, 1 + (hi_n - 1) + (far_n - 1) + 1)

    def cols(k):
        return pl.ds(k * piece, piece)

    def cross_copy(d, k):
        return pltpu.make_async_remote_copy(
            tokens.at[:, cols(k)], tok.at[t_me, :, cols(k)],
            cross_send.at[d - 1, k], cross_recv.at[d - 1, k],
            device_id={"tp": cross(d)}, device_id_type=MESH,
        )

    def pair_copy(k):
        return pltpu.make_async_remote_copy(
            tokens.at[:, cols(k)], tok.at[t_me, :, cols(k)],
            pair_send.at[k], pair_recv.at[k],
            device_id={"tp": pair}, device_id_type=MESH,
        )

    def relay_copy(d, k):
        source = lax.rem(hi - d + hi_n, hi_n) * lo_n + lo
        return pltpu.make_async_remote_copy(
            tok.at[source, :, cols(k)], tok.at[source, :, cols(k)],
            relay_send.at[d - 1, k], relay_recv.at[d - 1, k],
            device_id={"tp": pair}, device_id_type=MESH,
        )

    for k in range(chunks):
        for d in range(1, hi_n):
            cross_copy(d, k).start()
    for k in range(chunks):
        pair_copy(k).start()

    for load in loads[:3]:
        load.wait()
    build = 256

    def assemble(i, carry):
        span = pl.ds(pl.multiple_of(i * build, build), build)
        w_all[span, q_cols:] = w_kv[:, span].T
        return carry

    lax.fori_loop(0, width // build, assemble, 0)
    loads[3].wait()
    loads[4].wait()
    loads[5].wait()
    own.wait()
    wo_copy = pltpu.make_async_remote_copy(
        wo, wo_pair, wo_send, wo_recv, device_id={"tp": pair}, device_id_type=MESH
    )

    for k in range(chunks):
        for d in range(1, hi_n):
            cross_copy(d, k).wait_recv()
            relay_copy(d, k).start()
        pair_copy(k).wait_recv()
        for d in range(1, hi_n):
            relay_copy(d, k).wait_recv()
        here = tok[:, :, k * piece:(k + 1) * piece].reshape(local_rows, piece)
        part = jnp.dot(here, w_all[k * piece:(k + 1) * piece, :], preferred_element_type=jnp.float32)
        gate_part = lax.dot_general(
            w_g[:, k * piece:(k + 1) * piece], here, (((1,), (1,)), ((), ())),
            preferred_element_type=jnp.float32,
        )
        if k == 0:
            proj[...] = part
            logits[0:heads, :] = gate_part
        else:
            proj[...] += part
            logits[0:heads, :] += gate_part
    wo_copy.start()

    kv[me] = proj[:, q_cols:q_cols + 2 * key_cols].astype(jnp.bfloat16)
    scale = HEAD ** -0.5
    for h in range(heads):
        q = proj[:, h * HEAD:(h + 1) * HEAD].astype(jnp.bfloat16) * jnp.bfloat16(scale)
        q = jnp.concatenate([q, jnp.zeros((local_rows, LANES - HEAD), jnp.bfloat16)], axis=1)
        for g in range(hi_n):
            qs[g, h * group:(h + 1) * group, :] = q[g * group:(g + 1) * group]

    def column(d):
        return (
            pltpu.make_async_remote_copy(
                kv.at[me], kv.at[me], kv_send.at[d], kv_recv.at[me],
                device_id={"sp": d * span_n + side}, device_id_type=MESH,
            ),
            pltpu.make_async_remote_copy(
                cum.at[me], cum.at[me], cum_send.at[d], cum_recv.at[me],
                device_id={"sp": d * span_n + side}, device_id_type=MESH,
            ),
        )

    def across(r):
        return (
            pltpu.make_async_remote_copy(
                kv.at[r], kv.at[r], kv_side.at[lax.div(r, span_n)], kv_recv.at[r],
                device_id={"sp": mate}, device_id_type=MESH,
            ),
            pltpu.make_async_remote_copy(
                cum.at[r], cum.at[r], cum_side.at[lax.div(r, span_n)], cum_recv.at[r],
                device_id={"sp": mate}, device_id_type=MESH,
            ),
        )

    later = far_n - 1 - far

    def send_column(which, i, carry):
        column(far_n - 1 - i)[which].start()
        return carry

    lax.fori_loop(0, later, functools.partial(send_column, 0), 0)

    @pl.when(side == 0)
    def _():
        across(me)[0].start()

    row_of = lax.broadcasted_iota(jnp.int32, (8, local_rows), 0)
    u = jnp.where(row_of < heads, logits[...].astype(jnp.bfloat16).astype(jnp.float32), 0.0)
    for h in range(heads):
        u = jnp.where(row_of == h, u + bias[h], u)
    gates = jnp.minimum(u, 0.0) - jnp.log1p(jnp.exp(-jnp.abs(u)))
    upper = (
        lax.broadcasted_iota(jnp.int32, (local_rows, local_rows), 0)
        <= lax.broadcasted_iota(jnp.int32, (local_rows, local_rows), 1)
    )
    ones = jnp.where(upper, 1.0, 0.0).astype(jnp.bfloat16)
    g0 = gates.astype(jnp.bfloat16)
    r1 = gates - g0.astype(jnp.float32)
    g1 = r1.astype(jnp.bfloat16)
    g2 = (r1 - g1.astype(jnp.float32)).astype(jnp.bfloat16)
    total = jnp.dot(g2, ones, preferred_element_type=jnp.float32)
    total = total + jnp.dot(g1, ones, preferred_element_type=jnp.float32)
    total = total + jnp.dot(g0, ones, preferred_element_type=jnp.float32)
    own_sum[...] = jnp.broadcast_to(total[:, local_rows - 1:], (8, LANES))
    sum_copy = pltpu.make_async_remote_copy(
        own_sum, pair_sum, sum_send, sum_recv, device_id={"sp": mate}, device_id_type=MESH
    )
    sum_copy.start()

    halves = local_rows // LANES

    def lane_parts(x):
        return [x[:, j * LANES:(j + 1) * LANES] for j in range(halves)]

    def attend(g, kv_here, shift, first):
        s = lax.dot_general(
            qs[g], kv_here, (((1,), (1,)), ((), ())), preferred_element_type=jnp.float32
        )
        weights = []
        rescales = []
        for h in range(heads):
            here = slice(h * group, (h + 1) * group)
            x = s[here] + shift[h:h + 1, :]
            if first:
                allowed = (
                    lax.broadcasted_iota(jnp.int32, (group, local_rows), 1)
                    <= lax.broadcasted_iota(jnp.int32, (group, local_rows), 0) + g * group
                )
                x = jnp.where(allowed, x, masked_value)
            top = jnp.max(x, axis=1, keepdims=True)
            if first:
                new_peak = jnp.broadcast_to(top, (group, LANES))
            else:
                old_peak = peak[here, :]
                new_peak = jnp.maximum(old_peak, top)
                rescale = jnp.exp(old_peak - new_peak)
                rescales.append(rescale)
            p = [jnp.exp(part - new_peak) for part in lane_parts(x)]
            p_sum = functools.reduce(lambda a, b: a + b, p)
            weights.append(jnp.concatenate([part.astype(jnp.bfloat16) for part in p], axis=1))
            peak[here, :] = new_peak
            mass[here, :] = p_sum if first else mass[here, :] * rescale + p_sum
        term = jnp.dot(
            jnp.concatenate(weights, axis=0), kv_here, preferred_element_type=jnp.float32
        )
        for h in range(heads):
            here = slice(h * group, (h + 1) * group)
            if first:
                accum[here, :] = term[here]
            else:
                accum[here, :] = accum[here, :] * rescales[h] + term[here]

    def pass_over(g, fresh):
        attend(g, kv[me], -total, True)
        if fresh:
            sum_copy.wait_recv()
            start = jnp.where(side == 1, pair_sum[:, :1], 0.0)
            cum[me, :, 0:local_rows] = total + start
            cum[me, :, local_rows:] = own_sum[...] + pair_sum[...]
            lax.fori_loop(0, later, functools.partial(send_column, 1), 0)

            @pl.when(side == 0)
            def _():
                across(me)[1].start()

        start = jnp.where(side == 1, pair_sum[:, :1], 0.0)

        def same_side(i, base):
            r = (far - 1 - i) * span_n + side
            if fresh:
                for copy in across(r):
                    copy.wait_recv()
                for copy in across(r):
                    copy.start()
            base = base + cum[r, :, local_rows:local_rows + 1]
            attend(g, kv[r], base - cum[r, :, 0:local_rows], False)
            return base

        lax.fori_loop(0, far, same_side, start)

        @pl.when(side == 1)
        def _():
            if fresh:
                for copy in across(mate):
                    copy.wait_recv()
            attend(g, kv[mate], start - cum[mate, :, 0:local_rows], False)

        def other_side(i, base):
            r = (far - 1 - i) * span_n + 1 - side
            if fresh:
                for copy in across(r):
                    copy.wait_recv()
            base = base + cum[r, :, local_rows:local_rows + 1]
            attend(g, kv[r], base - cum[r, :, 0:local_rows], False)
            return base

        lax.fori_loop(0, far, other_side, start)

        for h in range(heads):
            here = slice(h * group, (h + 1) * group)
            denominator = jnp.sum(mass[here, :], axis=1, keepdims=True)
            done = (accum[here, key_cols:2 * key_cols] / denominator).astype(jnp.bfloat16)
            att[g, :, :, h * HEAD:(h + 1) * HEAD] = done.reshape(lo_n, rows, HEAD)

    def att_copy(g):
        return pltpu.make_async_remote_copy(
            att.at[g, 1 - lo], att_pair.at[g], att_send.at[g], att_recv.at[g],
            device_id={"tp": pair}, device_id_type=MESH,
        )

    def out_copy(d, k):
        span = pl.ds(k * out_piece, out_piece)
        return pltpu.make_async_remote_copy(
            outgoing.at[d - 1, :, span], incoming.at[d - 1, :, span],
            out_send.at[d - 1, k], out_recv.at[d - 1, k],
            device_id={"tp": cross(d)}, device_id_type=MESH,
        )

    def combined(g, k):
        span = slice(k * out_piece, (k + 1) * out_piece)
        a = jnp.dot(att[g, lo], wo[:, span], preferred_element_type=jnp.float32)
        b = jnp.dot(att_pair[g], wo_pair[:, span], preferred_element_type=jnp.float32)
        return (
            a.astype(jnp.bfloat16).astype(jnp.float32) + b.astype(jnp.bfloat16).astype(jnp.float32)
        )

    for d in list(range(1, hi_n)):
        g = lax.rem(hi + d, hi_n)
        pass_over(g, d == 1)
        att_copy(g).start()
        if d == 1:
            wo_copy.wait_recv()
        att_copy(g).wait_recv()
        for k in range(out_chunks):
            span = slice(k * out_piece, (k + 1) * out_piece)
            outgoing[d - 1, :, span] = combined(g, k).astype(jnp.bfloat16)
            out_copy(d, k).start()
    pass_over(hi, False)
    att_copy(hi).start()
    att_copy(hi).wait_recv()
    for k in range(out_chunks):
        keep[:, k * out_piece:(k + 1) * out_piece] = combined(hi, k)
    for k in range(out_chunks):
        span = slice(k * out_piece, (k + 1) * out_piece)
        value = keep[:, span]
        for d in range(1, hi_n):
            out_copy(d, k).wait_recv()
            value = value + incoming[d - 1, :, span].astype(jnp.float32)
        out[:, span] = value.astype(jnp.bfloat16)

    for k in range(chunks):
        for d in range(1, hi_n):
            cross_copy(d, k).wait_send()
            relay_copy(d, k).wait_send()
        pair_copy(k).wait_send()
    wo_copy.wait_send()
    for d in range(hi_n):
        att_copy(d).wait_send()
    for k in range(out_chunks):
        for d in range(1, hi_n):
            out_copy(d, k).wait_send()

    sum_copy.wait_send()

    @pl.when(side == 0)
    def _():
        for copy in across(me):
            copy.wait_send()

    def drain(i, carry):
        for copy in column(far_n - 1 - i):
            copy.wait_send()
        return carry

    lax.fori_loop(0, later, drain, 0)

    def drain_side(i, carry):
        for copy in across((far - 1 - i) * span_n + side):
            copy.wait_send()
        return carry

    lax.fori_loop(0, far, drain_side, 0)


def shards(tokens, w_query, w_key, w_value, w_gate, gate_bias, w_output):
    sp = lax.axis_size("sp")
    tp = lax.axis_size("tp")
    rows, width = tokens.shape
    local_rows = rows * tp
    q_cols, key_cols, heads = w_query.shape[1], w_key.shape[1], w_gate.shape[1]
    out_cols = w_output.shape[1]
    assert tp % 2 == 0 and sp % 2 == 0 and tp >= 4 and 2 * key_cols == LANES and key_cols == HEAD and heads <= 8
    hi_n = tp // 2
    chunks = 4
    out_chunks = 4
    bf, f32 = jnp.bfloat16, jnp.float32
    dma = pltpu.SemaphoreType.DMA
    hbm_spec = pl.BlockSpec(memory_space=pltpu.HBM)
    vmem_spec = pl.BlockSpec(memory_space=pltpu.VMEM)
    operands = (tokens, w_query, w_key.T, w_value.T, w_gate.T, gate_bias, w_output)
    return pl.pallas_call(
        functools.partial(kernel, sp, tp, chunks, out_chunks),
        out_shape=jax.ShapeDtypeStruct((rows, out_cols), bf),
        in_specs=[hbm_spec] * 7,
        out_specs=vmem_spec,
        scratch_shapes=[
            pltpu.VMEM((tp, rows, width), bf),
            pltpu.VMEM((width, q_cols + LANES), bf),
            pltpu.VMEM((LANES, width), bf),
            pltpu.VMEM((heads, width), bf),
            pltpu.VMEM(w_output.shape, bf),
            pltpu.VMEM(w_output.shape, bf),
            pltpu.VMEM((local_rows, q_cols + LANES), f32),
            pltpu.VMEM((8, local_rows), f32),
            pltpu.VMEM((hi_n, heads * 2 * rows, LANES), bf),
            pltpu.VMEM((sp, local_rows, LANES), bf),
            pltpu.VMEM((sp, 8, local_rows + LANES), f32),
            pltpu.VMEM((8, LANES), f32),
            pltpu.VMEM((8, LANES), f32),
            pltpu.VMEM((heads * 2 * rows, LANES), f32),
            pltpu.VMEM((heads * 2 * rows, LANES), f32),
            pltpu.VMEM((heads * 2 * rows, LANES), f32),
            pltpu.VMEM((hi_n, 2, rows, q_cols), bf),
            pltpu.VMEM((hi_n, rows, q_cols), bf),
            pltpu.VMEM((rows, out_cols), f32),
            pltpu.VMEM((hi_n - 1, rows, out_cols), bf),
            pltpu.VMEM((max(hi_n - 1, 1), rows, out_cols), bf),
            pltpu.SMEM((heads,), f32),
            dma((6,)),
            dma,
            dma((hi_n - 1, chunks)),
            dma((hi_n - 1, chunks)),
            dma((chunks,)),
            dma((chunks,)),
            dma((hi_n - 1, chunks)),
            dma((hi_n - 1, chunks)),
            dma,
            dma,
            dma((sp // 2,)),
            dma((sp,)),
            dma((sp // 2,)),
            dma((sp,)),
            dma((sp // 2,)),
            dma((sp // 2,)),
            dma,
            dma,
            dma((hi_n,)),
            dma((hi_n,)),
            dma((hi_n - 1, out_chunks)),
            dma((hi_n - 1, out_chunks)),
        ],
        compiler_params=pltpu.CompilerParams(
            collective_id=0, has_side_effects=True, vmem_limit_bytes=(20 << 20) + (sp << 17)
        ),
    )(*(pltpu.with_memory_space_constraint(x, pltpu.HBM) for x in operands))


def solution(mesh):
    return jax.shard_map(
        shards,
        mesh=mesh,
        in_specs=(
            P(("sp", "tp"), None),
            P(None, "tp"),
            P(None, "tp"),
            P(None, "tp"),
            P(None, "tp"),
            P("tp"),
            P("tp", None),
        ),
        out_specs=P(("sp", "tp"), None),
        check_vma=False,
    )
```

```python
import functools

import jax
import jax.numpy as jnp
from jax import lax
from jax.experimental import pallas as pl
from jax.experimental.pallas import tpu as pltpu
from jax.sharding import PartitionSpec as P

HEAD = 64
LANES = 128
masked_value = -1e30
MESH = pl.DeviceIdType.MESH


def kernel(
    sp, tp, chunks, out_chunks,
    tokens, w_query, w_key, w_value, w_gate, bias_in, w_output,
    out,
    tok, w_all, w_kv, w_g, wo, wo_pair, proj, logits, qs, kv, cum, own_sum, pair_sum,
    peak, mass, accum, att, att_pair, keep, outgoing, incoming, bias,
    local_sem, own_sem, cross_send, cross_recv, pair_send, pair_recv, relay_send, relay_recv,
    wo_send, wo_recv, kv_send, kv_recv, cum_send, cum_recv,
    kv_side, cum_side, sum_send, sum_recv,
    att_send, att_recv, out_send, out_recv,
):
    lo_n = 2
    hi_n = tp // lo_n
    me = lax.axis_index("sp")
    t_me = lax.axis_index("tp")
    hi, lo = lax.div(t_me, lo_n), lax.rem(t_me, lo_n)
    pair = hi * lo_n + (1 - lo)
    rows = tok.shape[1]
    local_rows = rows * tp
    width = tok.shape[2]
    q_cols = w_query.shape[1]
    heads = w_gate.shape[0]
    key_cols = w_key.shape[0]
    span_n = 2
    far_n = sp // span_n
    far, side = lax.div(me, span_n), lax.rem(me, span_n)
    mate = far * span_n + (1 - side)
    piece = width // chunks
    out_cols = w_output.shape[1]
    out_piece = out_cols // out_chunks
    group = lo_n * rows

    def cross(d):
        return lax.rem(hi + d, hi_n) * lo_n + lo

    loads = [
        pltpu.make_async_copy(w_key, w_kv.at[pl.ds(0, key_cols)], local_sem.at[0]),
        pltpu.make_async_copy(w_value, w_kv.at[pl.ds(key_cols, key_cols)], local_sem.at[1]),
        pltpu.make_async_copy(w_gate, w_g, local_sem.at[2]),
        pltpu.make_async_copy(w_query, w_all.at[:, pl.ds(0, q_cols)], local_sem.at[3]),
        pltpu.make_async_copy(w_output, wo, local_sem.at[4]),
        pltpu.make_async_copy(bias_in, bias, local_sem.at[5]),
    ]
    own = pltpu.make_async_copy(tokens, tok.at[t_me], own_sem)
    own.start()
    for load in loads:
        load.start()

    barrier = pltpu.get_barrier_semaphore()
    pl.semaphore_signal(barrier, inc=1, device_id={"tp": pair}, device_id_type=MESH)
    for d in range(1, hi_n):
        pl.semaphore_signal(barrier, inc=1, device_id={"tp": cross(d)}, device_id_type=MESH)

    def greet(d, carry):
        other = lax.rem(far + d, far_n) * span_n + side
        pl.semaphore_signal(barrier, inc=1, device_id={"sp": other}, device_id_type=MESH)
        return carry

    lax.fori_loop(1, far_n, greet, 0)
    pl.semaphore_signal(barrier, inc=1, device_id={"sp": mate}, device_id_type=MESH)
    pl.semaphore_wait(barrier, 1 + (hi_n - 1) + (far_n - 1) + 1)

    def cols(k):
        return pl.ds(k * piece, piece)

    def cross_copy(d, k):
        return pltpu.make_async_remote_copy(
            tok.at[t_me, :, cols(k)], tok.at[t_me, :, cols(k)],
            cross_send.at[d - 1, k], cross_recv.at[d - 1, k],
            device_id={"tp": cross(d)}, device_id_type=MESH,
        )

    def pair_copy(k):
        return pltpu.make_async_remote_copy(
            tok.at[t_me, :, cols(k)], tok.at[t_me, :, cols(k)],
            pair_send.at[k], pair_recv.at[k],
            device_id={"tp": pair}, device_id_type=MESH,
        )

    def relay_copy(d, k):
        source = lax.rem(hi - d + hi_n, hi_n) * lo_n + lo
        return pltpu.make_async_remote_copy(
            tok.at[source, :, cols(k)], tok.at[source, :, cols(k)],
            relay_send.at[d - 1, k], relay_recv.at[d - 1, k],
            device_id={"tp": pair}, device_id_type=MESH,
        )

    own.wait()
    for k in range(chunks):
        for d in range(1, hi_n):
            cross_copy(d, k).start()
    for k in range(chunks):
        pair_copy(k).start()

    for load in loads[:3]:
        load.wait()
    build = 256

    def assemble(i, carry):
        span = pl.ds(pl.multiple_of(i * build, build), build)
        w_all[span, q_cols:] = w_kv[:, span].T
        return carry

    lax.fori_loop(0, width // build, assemble, 0)
    loads[3].wait()
    loads[4].wait()
    loads[5].wait()
    wo_copy = pltpu.make_async_remote_copy(
        wo, wo_pair, wo_send, wo_recv, device_id={"tp": pair}, device_id_type=MESH
    )

    for k in range(chunks):
        for d in range(1, hi_n):
            cross_copy(d, k).wait_recv()
            relay_copy(d, k).start()
        pair_copy(k).wait_recv()
        for d in range(1, hi_n):
            relay_copy(d, k).wait_recv()
        here = tok[:, :, k * piece:(k + 1) * piece].reshape(local_rows, piece)
        part = jnp.dot(here, w_all[k * piece:(k + 1) * piece, :], preferred_element_type=jnp.float32)
        gate_part = lax.dot_general(
            w_g[:, k * piece:(k + 1) * piece], here, (((1,), (1,)), ((), ())),
            preferred_element_type=jnp.float32,
        )
        if k == 0:
            proj[...] = part
            logits[0:heads, :] = gate_part
        else:
            proj[...] += part
            logits[0:heads, :] += gate_part
    wo_copy.start()

    row_of = lax.broadcasted_iota(jnp.int32, (8, local_rows), 0)
    u = jnp.where(row_of < heads, logits[...].astype(jnp.bfloat16).astype(jnp.float32), 0.0)
    for h in range(heads):
        u = jnp.where(row_of == h, u + bias[h], u)
    gates = jnp.minimum(u, 0.0) - jnp.log1p(jnp.exp(-jnp.abs(u)))
    upper = (
        lax.broadcasted_iota(jnp.int32, (local_rows, local_rows), 0)
        <= lax.broadcasted_iota(jnp.int32, (local_rows, local_rows), 1)
    )
    ones = jnp.where(upper, 1.0, 0.0).astype(jnp.bfloat16)
    g0 = gates.astype(jnp.bfloat16)
    r1 = gates - g0.astype(jnp.float32)
    g1 = r1.astype(jnp.bfloat16)
    g2 = (r1 - g1.astype(jnp.float32)).astype(jnp.bfloat16)
    total = jnp.dot(g2, ones, preferred_element_type=jnp.float32)
    total = total + jnp.dot(g1, ones, preferred_element_type=jnp.float32)
    total = total + jnp.dot(g0, ones, preferred_element_type=jnp.float32)
    own_sum[...] = jnp.broadcast_to(total[:, local_rows - 1:], (8, LANES))
    sum_copy = pltpu.make_async_remote_copy(
        own_sum, pair_sum, sum_send, sum_recv, device_id={"sp": mate}, device_id_type=MESH
    )
    sum_copy.start()

    kv[me] = proj[:, q_cols:q_cols + 2 * key_cols].astype(jnp.bfloat16)
    scale = HEAD ** -0.5
    for h in range(heads):
        q = proj[:, h * HEAD:(h + 1) * HEAD].astype(jnp.bfloat16) * jnp.bfloat16(scale)
        q = jnp.concatenate([q, jnp.zeros((local_rows, LANES - HEAD), jnp.bfloat16)], axis=1)
        for g in range(hi_n):
            qs[g, h * group:(h + 1) * group, :] = q[g * group:(g + 1) * group]

    def column(d):
        return (
            pltpu.make_async_remote_copy(
                kv.at[me], kv.at[me], kv_send.at[d], kv_recv.at[me],
                device_id={"sp": d * span_n + side}, device_id_type=MESH,
            ),
            pltpu.make_async_remote_copy(
                cum.at[me], cum.at[me], cum_send.at[d], cum_recv.at[me],
                device_id={"sp": d * span_n + side}, device_id_type=MESH,
            ),
        )

    def across(r):
        return (
            pltpu.make_async_remote_copy(
                kv.at[r], kv.at[r], kv_side.at[lax.div(r, span_n)], kv_recv.at[r],
                device_id={"sp": mate}, device_id_type=MESH,
            ),
            pltpu.make_async_remote_copy(
                cum.at[r], cum.at[r], cum_side.at[lax.div(r, span_n)], cum_recv.at[r],
                device_id={"sp": mate}, device_id_type=MESH,
            ),
        )

    later = far_n - 1 - far

    def send_column(which, i, carry):
        column(far + 1 + i)[which].start()
        return carry

    lax.fori_loop(0, jnp.minimum(later, 1), functools.partial(send_column, 0), 0)

    @pl.when(side == 0)
    def _():
        across(me)[0].start()

    halves = local_rows // LANES

    def lane_parts(x):
        return [x[:, j * LANES:(j + 1) * LANES] for j in range(halves)]

    def attend(g, kv_here, shift, first):
        s = lax.dot_general(
            qs[g], kv_here, (((1,), (1,)), ((), ())), preferred_element_type=jnp.float32
        )
        weights = []
        rescales = []
        for h in range(heads):
            here = slice(h * group, (h + 1) * group)
            x = s[here] + shift[h:h + 1, :]
            if first:
                allowed = (
                    lax.broadcasted_iota(jnp.int32, (group, local_rows), 1)
                    <= lax.broadcasted_iota(jnp.int32, (group, local_rows), 0) + g * group
                )
                x = jnp.where(allowed, x, masked_value)
            top = jnp.max(x, axis=1, keepdims=True)
            if first:
                new_peak = jnp.broadcast_to(top, (group, LANES))
            else:
                old_peak = peak[here, :]
                new_peak = jnp.maximum(old_peak, top)
                rescale = jnp.exp(old_peak - new_peak)
                rescales.append(rescale)
            p = [jnp.exp(part - new_peak) for part in lane_parts(x)]
            p_sum = functools.reduce(lambda a, b: a + b, p)
            weights.append(jnp.concatenate([part.astype(jnp.bfloat16) for part in p], axis=1))
            peak[here, :] = new_peak
            mass[here, :] = p_sum if first else mass[here, :] * rescale + p_sum
        term = jnp.dot(
            jnp.concatenate(weights, axis=0), kv_here, preferred_element_type=jnp.float32
        )
        for h in range(heads):
            here = slice(h * group, (h + 1) * group)
            if first:
                accum[here, :] = term[here]
            else:
                accum[here, :] = accum[here, :] * rescales[h] + term[here]

    def pass_over(g, fresh):
        attend(g, kv[me], -total, True)
        if fresh:
            sum_copy.wait_recv()
            start = jnp.where(side == 1, pair_sum[:, :1], 0.0)
            cum[me, :, 0:local_rows] = total + start
            cum[me, :, local_rows:] = own_sum[...] + pair_sum[...]
            lax.fori_loop(0, later, functools.partial(send_column, 1), 0)
            lax.fori_loop(1, later, functools.partial(send_column, 0), 0)

            @pl.when(side == 0)
            def _():
                across(me)[1].start()

        start = jnp.where(side == 1, pair_sum[:, :1], 0.0)

        def same_side(i, base):
            r = (far - 1 - i) * span_n + side
            if fresh:
                for copy in across(r):
                    copy.wait_recv()
                for copy in across(r):
                    copy.start()
            base = base + cum[r, :, local_rows:local_rows + 1]
            attend(g, kv[r], base - cum[r, :, 0:local_rows], False)
            return base

        lax.fori_loop(0, far, same_side, start)

        @pl.when(side == 1)
        def _():
            if fresh:
                for copy in across(mate):
                    copy.wait_recv()
            attend(g, kv[mate], start - cum[mate, :, 0:local_rows], False)

        def other_side(i, base):
            r = (far - 1 - i) * span_n + 1 - side
            if fresh:
                for copy in across(r):
                    copy.wait_recv()
            base = base + cum[r, :, local_rows:local_rows + 1]
            attend(g, kv[r], base - cum[r, :, 0:local_rows], False)
            return base

        lax.fori_loop(0, far, other_side, start)

        for h in range(heads):
            here = slice(h * group, (h + 1) * group)
            denominator = jnp.sum(mass[here, :], axis=1, keepdims=True)
            done = (accum[here, key_cols:2 * key_cols] / denominator).astype(jnp.bfloat16)
            att[g, :, :, h * HEAD:(h + 1) * HEAD] = done.reshape(lo_n, rows, HEAD)

    def att_copy(g):
        return pltpu.make_async_remote_copy(
            att.at[g, 1 - lo], att_pair.at[g], att_send.at[g], att_recv.at[g],
            device_id={"tp": pair}, device_id_type=MESH,
        )

    def out_copy(d, k):
        span = pl.ds(k * out_piece, out_piece)
        return pltpu.make_async_remote_copy(
            outgoing.at[d - 1, :, span], incoming.at[d - 1, :, span],
            out_send.at[d - 1, k], out_recv.at[d - 1, k],
            device_id={"tp": cross(d)}, device_id_type=MESH,
        )

    def combined(g, k):
        span = slice(k * out_piece, (k + 1) * out_piece)
        a = jnp.dot(att[g, lo], wo[:, span], preferred_element_type=jnp.float32)
        b = jnp.dot(att_pair[g], wo_pair[:, span], preferred_element_type=jnp.float32)
        return (
            a.astype(jnp.bfloat16).astype(jnp.float32) + b.astype(jnp.bfloat16).astype(jnp.float32)
        )

    for d in list(range(1, hi_n)):
        g = lax.rem(hi + d, hi_n)
        pass_over(g, d == 1)
        att_copy(g).start()
        if d == 1:
            wo_copy.wait_recv()
        att_copy(g).wait_recv()
        for k in range(out_chunks):
            span = slice(k * out_piece, (k + 1) * out_piece)
            outgoing[d - 1, :, span] = combined(g, k).astype(jnp.bfloat16)
            out_copy(d, k).start()
    pass_over(hi, False)
    att_copy(hi).start()
    att_copy(hi).wait_recv()
    for k in range(out_chunks):
        keep[:, k * out_piece:(k + 1) * out_piece] = combined(hi, k)
    for k in range(out_chunks):
        span = slice(k * out_piece, (k + 1) * out_piece)
        value = keep[:, span]
        for d in range(1, hi_n):
            out_copy(d, k).wait_recv()
            value = value + incoming[d - 1, :, span].astype(jnp.float32)
        out[:, span] = value.astype(jnp.bfloat16)

    for k in range(chunks):
        for d in range(1, hi_n):
            cross_copy(d, k).wait_send()
            relay_copy(d, k).wait_send()
        pair_copy(k).wait_send()
    wo_copy.wait_send()
    for d in range(hi_n):
        att_copy(d).wait_send()
    for k in range(out_chunks):
        for d in range(1, hi_n):
            out_copy(d, k).wait_send()

    sum_copy.wait_send()

    @pl.when(side == 0)
    def _():
        for copy in across(me):
            copy.wait_send()

    def drain(i, carry):
        for copy in column(far_n - 1 - i):
            copy.wait_send()
        return carry

    lax.fori_loop(0, later, drain, 0)

    def drain_side(i, carry):
        for copy in across((far - 1 - i) * span_n + side):
            copy.wait_send()
        return carry

    lax.fori_loop(0, far, drain_side, 0)


def shards(tokens, w_query, w_key, w_value, w_gate, gate_bias, w_output):
    sp = lax.axis_size("sp")
    tp = lax.axis_size("tp")
    rows, width = tokens.shape
    local_rows = rows * tp
    q_cols, key_cols, heads = w_query.shape[1], w_key.shape[1], w_gate.shape[1]
    out_cols = w_output.shape[1]
    assert tp % 2 == 0 and sp % 2 == 0 and tp >= 4 and 2 * key_cols == LANES and key_cols == HEAD and heads <= 8
    hi_n = tp // 2
    chunks = 8
    out_chunks = 8
    bf, f32 = jnp.bfloat16, jnp.float32
    dma = pltpu.SemaphoreType.DMA
    hbm_spec = pl.BlockSpec(memory_space=pltpu.HBM)
    vmem_spec = pl.BlockSpec(memory_space=pltpu.VMEM)
    operands = (tokens, w_query, w_key.T, w_value.T, w_gate.T, gate_bias, w_output)
    return pl.pallas_call(
        functools.partial(kernel, sp, tp, chunks, out_chunks),
        out_shape=jax.ShapeDtypeStruct((rows, out_cols), bf),
        in_specs=[hbm_spec] * 7,
        out_specs=vmem_spec,
        scratch_shapes=[
            pltpu.VMEM((tp, rows, width), bf),
            pltpu.VMEM((width, q_cols + LANES), bf),
            pltpu.VMEM((LANES, width), bf),
            pltpu.VMEM((heads, width), bf),
            pltpu.VMEM(w_output.shape, bf),
            pltpu.VMEM(w_output.shape, bf),
            pltpu.VMEM((local_rows, q_cols + LANES), f32),
            pltpu.VMEM((8, local_rows), f32),
            pltpu.VMEM((hi_n, heads * 2 * rows, LANES), bf),
            pltpu.VMEM((sp, local_rows, LANES), bf),
            pltpu.VMEM((sp, 8, local_rows + LANES), f32),
            pltpu.VMEM((8, LANES), f32),
            pltpu.VMEM((8, LANES), f32),
            pltpu.VMEM((heads * 2 * rows, LANES), f32),
            pltpu.VMEM((heads * 2 * rows, LANES), f32),
            pltpu.VMEM((heads * 2 * rows, LANES), f32),
            pltpu.VMEM((hi_n, 2, rows, q_cols), bf),
            pltpu.VMEM((hi_n, rows, q_cols), bf),
            pltpu.VMEM((rows, out_cols), f32),
            pltpu.VMEM((hi_n - 1, rows, out_cols), bf),
            pltpu.VMEM((max(hi_n - 1, 1), rows, out_cols), bf),
            pltpu.SMEM((heads,), f32),
            dma((6,)),
            dma,
            dma((hi_n - 1, chunks)),
            dma((hi_n - 1, chunks)),
            dma((chunks,)),
            dma((chunks,)),
            dma((hi_n - 1, chunks)),
            dma((hi_n - 1, chunks)),
            dma,
            dma,
            dma((sp // 2,)),
            dma((sp,)),
            dma((sp // 2,)),
            dma((sp,)),
            dma((sp // 2,)),
            dma((sp // 2,)),
            dma,
            dma,
            dma((hi_n,)),
            dma((hi_n,)),
            dma((hi_n - 1, out_chunks)),
            dma((hi_n - 1, out_chunks)),
        ],
        compiler_params=pltpu.CompilerParams(
            collective_id=0, has_side_effects=True, vmem_limit_bytes=(20 << 20) + (sp << 17)
        ),
    )(*(pltpu.with_memory_space_constraint(x, pltpu.HBM) for x in operands))


def solution(mesh):
    return jax.shard_map(
        shards,
        mesh=mesh,
        in_specs=(
            P(("sp", "tp"), None),
            P(None, "tp"),
            P(None, "tp"),
            P(None, "tp"),
            P(None, "tp"),
            P("tp"),
            P("tp", None),
        ),
        out_specs=P(("sp", "tp"), None),
        check_vma=False,
    )
```

```python
import functools

import jax
import jax.numpy as jnp
from jax import lax
from jax.experimental import pallas as pl
from jax.experimental.pallas import tpu as pltpu
from jax.sharding import PartitionSpec as P

HEAD = 64
LANES = 128
masked_value = -1e30
MESH = pl.DeviceIdType.MESH


def kernel(
    sp, tp, chunks, out_chunks,
    tokens, w_query, w_key, w_value, w_gate, bias_in, w_output,
    out,
    tok, w_all, w_kv, w_g, wo, wo_pair, proj, logits, qs, kv, cum, own_sum, pair_sum,
    peak, mass, accum, att, att_pair, keep, outgoing, incoming, bias,
    local_sem, own_sem, cross_send, cross_recv, pair_send, pair_recv, relay_send, relay_recv,
    wo_send, wo_recv, kv_send, kv_recv, cum_send, cum_recv,
    kv_side, cum_side, sum_send, sum_recv,
    att_send, att_recv, out_send, out_recv,
):
    lo_n = 2
    hi_n = tp // lo_n
    me = lax.axis_index("sp")
    t_me = lax.axis_index("tp")
    hi, lo = lax.div(t_me, lo_n), lax.rem(t_me, lo_n)
    pair = hi * lo_n + (1 - lo)
    rows = tok.shape[1]
    local_rows = rows * tp
    width = tok.shape[2]
    q_cols = w_query.shape[1]
    heads = w_gate.shape[0]
    key_cols = w_key.shape[0]
    span_n = 2
    far_n = sp // span_n
    far, side = lax.div(me, span_n), lax.rem(me, span_n)
    mate = far * span_n + (1 - side)
    piece = width // chunks
    out_cols = w_output.shape[1]
    out_piece = out_cols // out_chunks
    group = lo_n * rows
    half = 4

    def cross(d):
        return lax.rem(hi + d, hi_n) * lo_n + lo

    loads = [
        pltpu.make_async_copy(w_key, w_kv.at[pl.ds(0, key_cols)], local_sem.at[0]),
        pltpu.make_async_copy(w_value, w_kv.at[pl.ds(key_cols, key_cols)], local_sem.at[1]),
        pltpu.make_async_copy(w_gate, w_g, local_sem.at[2]),
        pltpu.make_async_copy(w_query, w_all.at[:, pl.ds(0, q_cols)], local_sem.at[3]),
        pltpu.make_async_copy(w_output, wo, local_sem.at[4]),
        pltpu.make_async_copy(bias_in, bias, local_sem.at[5]),
    ]
    own = pltpu.make_async_copy(tokens, tok.at[t_me], own_sem)
    own.start()
    for load in loads:
        load.start()

    barrier = pltpu.get_barrier_semaphore()
    pl.semaphore_signal(barrier, inc=1, device_id={"tp": pair}, device_id_type=MESH)
    for d in range(1, hi_n):
        pl.semaphore_signal(barrier, inc=1, device_id={"tp": cross(d)}, device_id_type=MESH)

    def greet(d, carry):
        other = lax.rem(far + d, far_n) * span_n + side
        pl.semaphore_signal(barrier, inc=1, device_id={"sp": other}, device_id_type=MESH)
        return carry

    lax.fori_loop(1, far_n, greet, 0)
    pl.semaphore_signal(barrier, inc=1, device_id={"sp": mate}, device_id_type=MESH)
    pl.semaphore_wait(barrier, 1 + (hi_n - 1) + (far_n - 1) + 1)

    def cols(k):
        return pl.ds(k * piece, piece)

    def cross_copy(d, k):
        return pltpu.make_async_remote_copy(
            tok.at[t_me, :, cols(k)], tok.at[t_me, :, cols(k)],
            cross_send.at[d - 1, k], cross_recv.at[d - 1, k],
            device_id={"tp": cross(d)}, device_id_type=MESH,
        )

    def pair_copy(k):
        return pltpu.make_async_remote_copy(
            tok.at[t_me, :, cols(k)], tok.at[t_me, :, cols(k)],
            pair_send.at[k], pair_recv.at[k],
            device_id={"tp": pair}, device_id_type=MESH,
        )

    def relay_copy(d, k):
        source = lax.rem(hi - d + hi_n, hi_n) * lo_n + lo
        return pltpu.make_async_remote_copy(
            tok.at[source, :, cols(k)], tok.at[source, :, cols(k)],
            relay_send.at[d - 1, k], relay_recv.at[d - 1, k],
            device_id={"tp": pair}, device_id_type=MESH,
        )

    own.wait()
    for k in range(chunks):
        for d in range(1, hi_n):
            cross_copy(d, k).start()
    for k in range(chunks):
        pair_copy(k).start()

    for load in loads[:3]:
        load.wait()
    build = 256

    def assemble(i, carry):
        span = pl.ds(pl.multiple_of(i * build, build), build)
        w_all[span, q_cols:] = w_kv[:, span].T
        return carry

    lax.fori_loop(0, width // build, assemble, 0)
    loads[3].wait()
    loads[4].wait()
    loads[5].wait()
    wo_copy = pltpu.make_async_remote_copy(
        wo, wo_pair, wo_send, wo_recv, device_id={"tp": pair}, device_id_type=MESH
    )

    for k in range(chunks):
        for d in range(1, hi_n):
            cross_copy(d, k).wait_recv()
            relay_copy(d, k).start()
        pair_copy(k).wait_recv()
        for d in range(1, hi_n):
            relay_copy(d, k).wait_recv()
        here = tok[:, :, k * piece:(k + 1) * piece].reshape(local_rows, piece)
        part = jnp.dot(here, w_all[k * piece:(k + 1) * piece, :], preferred_element_type=jnp.float32)
        gate_part = lax.dot_general(
            w_g[:, k * piece:(k + 1) * piece], here, (((1,), (1,)), ((), ())),
            preferred_element_type=jnp.float32,
        )
        if k == 0:
            proj[...] = part
            logits[0:heads, :] = gate_part
        else:
            proj[...] += part
            logits[0:heads, :] += gate_part
    wo_copy.start()

    row_of = lax.broadcasted_iota(jnp.int32, (8, local_rows), 0)
    u = jnp.where(row_of < heads, logits[...].astype(jnp.bfloat16).astype(jnp.float32), 0.0)
    for h in range(heads):
        u = jnp.where(row_of == h, u + bias[h], u)
    gates = jnp.minimum(u, 0.0) - jnp.log1p(jnp.exp(-jnp.abs(u)))
    upper = (
        lax.broadcasted_iota(jnp.int32, (local_rows, local_rows), 0)
        <= lax.broadcasted_iota(jnp.int32, (local_rows, local_rows), 1)
    )
    ones = jnp.where(upper, 1.0, 0.0).astype(jnp.bfloat16)
    g0 = gates.astype(jnp.bfloat16)
    r1 = gates - g0.astype(jnp.float32)
    g1 = r1.astype(jnp.bfloat16)
    g2 = (r1 - g1.astype(jnp.float32)).astype(jnp.bfloat16)
    total = jnp.dot(g2, ones, preferred_element_type=jnp.float32)
    total = total + jnp.dot(g1, ones, preferred_element_type=jnp.float32)
    total = total + jnp.dot(g0, ones, preferred_element_type=jnp.float32)
    own_sum[...] = jnp.broadcast_to(total[:, local_rows - 1:], (8, LANES))
    sum_copy = pltpu.make_async_remote_copy(
        own_sum, pair_sum, sum_send, sum_recv, device_id={"sp": mate}, device_id_type=MESH
    )
    sum_copy.start()

    kv[me] = proj[:, q_cols:q_cols + 2 * key_cols].astype(jnp.bfloat16)
    scale = HEAD ** -0.5
    for h in range(heads):
        q = proj[:, h * HEAD:(h + 1) * HEAD].astype(jnp.bfloat16) * jnp.bfloat16(scale)
        q = jnp.concatenate([q, jnp.zeros((local_rows, LANES - HEAD), jnp.bfloat16)], axis=1)
        for g in range(hi_n):
            qs[g, h * group:(h + 1) * group, :] = q[g * group:(g + 1) * group]

    def column(d):
        return (
            pltpu.make_async_remote_copy(
                kv.at[me], kv.at[me], kv_send.at[d], kv_recv.at[me],
                device_id={"sp": d * span_n + side}, device_id_type=MESH,
            ),
            pltpu.make_async_remote_copy(
                cum.at[me], cum.at[me], cum_send.at[d], cum_recv.at[me],
                device_id={"sp": d * span_n + side}, device_id_type=MESH,
            ),
        )

    def across(r):
        return (
            pltpu.make_async_remote_copy(
                kv.at[r], kv.at[r], kv_side.at[lax.div(r, span_n)], kv_recv.at[r],
                device_id={"sp": mate}, device_id_type=MESH,
            ),
            pltpu.make_async_remote_copy(
                cum.at[r], cum.at[r], cum_side.at[lax.div(r, span_n)], cum_recv.at[r],
                device_id={"sp": mate}, device_id_type=MESH,
            ),
        )

    later = far_n - 1 - far

    def send_column(which, i, carry):
        column(far + 1 + i)[which].start()
        return carry

    lax.fori_loop(0, jnp.minimum(later, 1), functools.partial(send_column, 0), 0)

    @pl.when(side == 0)
    def _():
        across(me)[0].start()

    halves = local_rows // LANES

    def lane_parts(x):
        return [x[:, j * LANES:(j + 1) * LANES] for j in range(halves)]

    def attend(g, kv_here, shift, first):
        s = lax.dot_general(
            qs[g], kv_here, (((1,), (1,)), ((), ())), preferred_element_type=jnp.float32
        )
        weights = []
        rescales = []
        for h in range(heads):
            here = slice(h * group, (h + 1) * group)
            x = s[here] + shift[h:h + 1, :]
            if first:
                allowed = (
                    lax.broadcasted_iota(jnp.int32, (group, local_rows), 1)
                    <= lax.broadcasted_iota(jnp.int32, (group, local_rows), 0) + g * group
                )
                x = jnp.where(allowed, x, masked_value)
            top = jnp.max(x, axis=1, keepdims=True)
            if first:
                new_peak = jnp.broadcast_to(top, (group, LANES))
            else:
                old_peak = peak[here, :]
                new_peak = jnp.maximum(old_peak, top)
                rescale = jnp.exp(old_peak - new_peak)
                rescales.append(rescale)
            p = [jnp.exp(part - new_peak) for part in lane_parts(x)]
            p_sum = functools.reduce(lambda a, b: a + b, p)
            weights.append(jnp.concatenate([part.astype(jnp.bfloat16) for part in p], axis=1))
            peak[here, :] = new_peak
            mass[here, :] = p_sum if first else mass[here, :] * rescale + p_sum
        term = jnp.dot(
            jnp.concatenate(weights, axis=0), kv_here, preferred_element_type=jnp.float32
        )
        for h in range(heads):
            here = slice(h * group, (h + 1) * group)
            if first:
                accum[here, :] = term[here]
            else:
                accum[here, :] = accum[here, :] * rescales[h] + term[here]

    def pass_over(g, fresh):
        attend(g, kv[me], -total, True)
        if fresh:
            sum_copy.wait_recv()
            start = jnp.where(side == 1, pair_sum[:, :1], 0.0)
            both_sums = jnp.broadcast_to((own_sum[...] + pair_sum[...])[:, :1], (8, local_rows))
            cum[me] = jnp.concatenate([(total + start)[:half], both_sums[:half]], axis=0)
            lax.fori_loop(0, later, functools.partial(send_column, 1), 0)
            lax.fori_loop(1, later, functools.partial(send_column, 0), 0)

            @pl.when(side == 0)
            def _():
                across(me)[1].start()

        start = jnp.where(side == 1, pair_sum[0:half, :1], 0.0)

        def same_side(i, base):
            r = (far - 1 - i) * span_n + side
            if fresh:
                for copy in across(r):
                    copy.wait_recv()
                for copy in across(r):
                    copy.start()
            base = base + cum[r, half:, 0:1]
            attend(g, kv[r], base - cum[r, 0:half, :], False)
            return base

        lax.fori_loop(0, far, same_side, start)

        @pl.when(side == 1)
        def _():
            if fresh:
                for copy in across(mate):
                    copy.wait_recv()
            attend(g, kv[mate], start - cum[mate, 0:half, :], False)

        def other_side(i, base):
            r = (far - 1 - i) * span_n + 1 - side
            if fresh:
                for copy in across(r):
                    copy.wait_recv()
            base = base + cum[r, half:, 0:1]
            attend(g, kv[r], base - cum[r, 0:half, :], False)
            return base

        lax.fori_loop(0, far, other_side, start)

        for h in range(heads):
            here = slice(h * group, (h + 1) * group)
            denominator = jnp.sum(mass[here, :], axis=1, keepdims=True)
            done = (accum[here, key_cols:2 * key_cols] / denominator).astype(jnp.bfloat16)
            att[g, :, :, h * HEAD:(h + 1) * HEAD] = done.reshape(lo_n, rows, HEAD)

    def att_copy(g):
        return pltpu.make_async_remote_copy(
            att.at[g, 1 - lo], att_pair.at[g], att_send.at[g], att_recv.at[g],
            device_id={"tp": pair}, device_id_type=MESH,
        )

    def out_copy(d, k):
        span = pl.ds(k * out_piece, out_piece)
        return pltpu.make_async_remote_copy(
            outgoing.at[d - 1, :, span], incoming.at[d - 1, :, span],
            out_send.at[d - 1, k], out_recv.at[d - 1, k],
            device_id={"tp": cross(d)}, device_id_type=MESH,
        )

    def combined(g, k):
        span = slice(k * out_piece, (k + 1) * out_piece)
        a = jnp.dot(att[g, lo], wo[:, span], preferred_element_type=jnp.float32)
        b = jnp.dot(att_pair[g], wo_pair[:, span], preferred_element_type=jnp.float32)
        return (
            a.astype(jnp.bfloat16).astype(jnp.float32) + b.astype(jnp.bfloat16).astype(jnp.float32)
        )

    for d in list(range(1, hi_n)):
        g = lax.rem(hi + d, hi_n)
        pass_over(g, d == 1)
        att_copy(g).start()
        if d == 1:
            wo_copy.wait_recv()
        att_copy(g).wait_recv()
        for k in range(out_chunks):
            span = slice(k * out_piece, (k + 1) * out_piece)
            outgoing[d - 1, :, span] = combined(g, k).astype(jnp.bfloat16)
            out_copy(d, k).start()
    pass_over(hi, False)
    att_copy(hi).start()
    att_copy(hi).wait_recv()
    for k in range(out_chunks):
        keep[:, k * out_piece:(k + 1) * out_piece] = combined(hi, k)
    for k in range(out_chunks):
        span = slice(k * out_piece, (k + 1) * out_piece)
        value = keep[:, span]
        for d in range(1, hi_n):
            out_copy(d, k).wait_recv()
            value = value + incoming[d - 1, :, span].astype(jnp.float32)
        out[:, span] = value.astype(jnp.bfloat16)

    for k in range(chunks):
        for d in range(1, hi_n):
            cross_copy(d, k).wait_send()
            relay_copy(d, k).wait_send()
        pair_copy(k).wait_send()
    wo_copy.wait_send()
    for d in range(hi_n):
        att_copy(d).wait_send()
    for k in range(out_chunks):
        for d in range(1, hi_n):
            out_copy(d, k).wait_send()

    sum_copy.wait_send()

    @pl.when(side == 0)
    def _():
        for copy in across(me):
            copy.wait_send()

    def drain(i, carry):
        for copy in column(far_n - 1 - i):
            copy.wait_send()
        return carry

    lax.fori_loop(0, later, drain, 0)

    def drain_side(i, carry):
        for copy in across((far - 1 - i) * span_n + side):
            copy.wait_send()
        return carry

    lax.fori_loop(0, far, drain_side, 0)


def shards(tokens, w_query, w_key, w_value, w_gate, gate_bias, w_output):
    sp = lax.axis_size("sp")
    tp = lax.axis_size("tp")
    rows, width = tokens.shape
    local_rows = rows * tp
    q_cols, key_cols, heads = w_query.shape[1], w_key.shape[1], w_gate.shape[1]
    out_cols = w_output.shape[1]
    assert tp % 2 == 0 and sp % 2 == 0 and tp >= 4 and 2 * key_cols == LANES and key_cols == HEAD and heads <= 4
    hi_n = tp // 2
    chunks = 2
    out_chunks = 2
    bf, f32 = jnp.bfloat16, jnp.float32
    dma = pltpu.SemaphoreType.DMA
    hbm_spec = pl.BlockSpec(memory_space=pltpu.HBM)
    vmem_spec = pl.BlockSpec(memory_space=pltpu.VMEM)
    operands = (tokens, w_query, w_key.T, w_value.T, w_gate.T, gate_bias, w_output)
    return pl.pallas_call(
        functools.partial(kernel, sp, tp, chunks, out_chunks),
        out_shape=jax.ShapeDtypeStruct((rows, out_cols), bf),
        in_specs=[hbm_spec] * 7,
        out_specs=vmem_spec,
        scratch_shapes=[
            pltpu.VMEM((tp, rows, width), bf),
            pltpu.VMEM((width, q_cols + LANES), bf),
            pltpu.VMEM((LANES, width), bf),
            pltpu.VMEM((heads, width), bf),
            pltpu.VMEM(w_output.shape, bf),
            pltpu.VMEM(w_output.shape, bf),
            pltpu.VMEM((local_rows, q_cols + LANES), f32),
            pltpu.VMEM((8, local_rows), f32),
            pltpu.VMEM((hi_n, heads * 2 * rows, LANES), bf),
            pltpu.VMEM((sp, local_rows, LANES), bf),
            pltpu.VMEM((sp, 8, local_rows), f32),
            pltpu.VMEM((8, LANES), f32),
            pltpu.VMEM((8, LANES), f32),
            pltpu.VMEM((heads * 2 * rows, LANES), f32),
            pltpu.VMEM((heads * 2 * rows, LANES), f32),
            pltpu.VMEM((heads * 2 * rows, LANES), f32),
            pltpu.VMEM((hi_n, 2, rows, q_cols), bf),
            pltpu.VMEM((hi_n, rows, q_cols), bf),
            pltpu.VMEM((rows, out_cols), f32),
            pltpu.VMEM((hi_n - 1, rows, out_cols), bf),
            pltpu.VMEM((max(hi_n - 1, 1), rows, out_cols), bf),
            pltpu.SMEM((heads,), f32),
            dma((6,)),
            dma,
            dma((hi_n - 1, chunks)),
            dma((hi_n - 1, chunks)),
            dma((chunks,)),
            dma((chunks,)),
            dma((hi_n - 1, chunks)),
            dma((hi_n - 1, chunks)),
            dma,
            dma,
            dma((sp // 2,)),
            dma((sp,)),
            dma((sp // 2,)),
            dma((sp,)),
            dma((sp // 2,)),
            dma((sp // 2,)),
            dma,
            dma,
            dma((hi_n,)),
            dma((hi_n,)),
            dma((hi_n - 1, out_chunks)),
            dma((hi_n - 1, out_chunks)),
        ],
        compiler_params=pltpu.CompilerParams(
            collective_id=0, has_side_effects=True, vmem_limit_bytes=(20 << 20) + (sp << 17)
        ),
    )(*(pltpu.with_memory_space_constraint(x, pltpu.HBM) for x in operands))


def solution(mesh):
    return jax.shard_map(
        shards,
        mesh=mesh,
        in_specs=(
            P(("sp", "tp"), None),
            P(None, "tp"),
            P(None, "tp"),
            P(None, "tp"),
            P(None, "tp"),
            P("tp"),
            P("tp", None),
        ),
        out_specs=P(("sp", "tp"), None),
        check_vma=False,
    )
```
